256 devices in a mesh: fs: 32 (over z, y), tp: 8 (over x, core).
Axes of the slice: x: 4, y: 4, z: 8, core: 2. Of those that a mesh axis runs over, the one named last changes fastest.
Arguments:
- normed_input: bfloat16 [16384, 2048], P('fs', 'tp'), may hold values from -6 to 6
- cotangent: bfloat16 [16384, 2048], P('fs', 'tp'), may hold values from -6 to 6
- up_weight: bfloat16 [2048, 8192], P('fs', 'tp'), may hold values from -0.125 to 0.125
- down_weight: bfloat16 [8192, 2048], P('tp', 'fs'), may hold values from -0.0625 to 0.0625
Outputs:
- input_grad: bfloat16 [16384, 2048], P('fs', 'tp')
- up_grad: float32 [2048, 8192], P('fs', 'tp')
- down_grad: float32 [8192, 2048], P('tp', 'fs')
The draws below stay inside these ranges and needn't reach their ends.
All inputs are finite; a program needn't handle non-finite values.
Results may differ from the reference program's by a relative error of at most 0.018.
Values may be sent and summed in bfloat16 or wider, within the bound.
No kernel may reach another device: no remote copies, remote signals or barrier semaphores. Data moves between devices by JAX's collectives and lax.ppermute only.
A program may use at most 64 MiB of HBM per device.

```python
import jax
import jax.numpy as jnp
from jax import lax

D = 2048
FF = 8192
TOKENS = 16384
FF_BLOCKS = 8


def strengthened(array, key, source, target, blocks, factor):
    owner, partner = [(jnp.arange(array.shape[axis_at]) // (array.shape[axis_at] // blocks)).reshape([-1 if axis == axis_at else 1 for axis in range(array.ndim)]) for axis_at in (source, target)]
    chosen = jax.random.permutation(key, blocks)[partner]
    strong = (owner == chosen) | (owner == (partner + blocks // 2) % blocks)
    return jnp.where(strong, factor * array, array)


def steps_of(stream_key, extent, shards, smallest, top_value):
    gain = 1.0
    for position, shards_of in shards:
        steps = jax.random.uniform(jax.random.fold_in(jax.random.fold_in(stream_key, 6), position), (shards_of,), jnp.float32, smallest / len(shards), top_value / len(shards))
        gain = gain * jnp.repeat(jnp.exp(steps), extent[position] // shards_of).reshape((-1,) + (1,) * (len(extent) - 1 - position))
    return gain


def bell_draw(stream_key, dims, spread, limit, pieces=(), kind=jnp.bfloat16):
    array = spread * jax.random.normal(stream_key, dims, jnp.float32)
    if pieces:
        array = array * steps_of(stream_key, dims, pieces, -0.22, 0.18)
    return jnp.clip(array, -limit, limit).astype(kind)


def heavy_noise(own_key, extent, spread, limit, cuts, heavy, kind=jnp.bfloat16):
    result = spread * jax.random.normal(own_key, extent, jnp.float32)
    if cuts:
        result = result * steps_of(own_key, extent, cuts, -0.22, 0.18)
    return jnp.clip(strengthened(result, jax.random.fold_in(own_key, 3), *heavy), -limit, limit).astype(kind)


def setup_inputs(seed: int = 0) -> dict:
    splits = jax.random.split(jax.random.key(seed), 5)
    normed_input = heavy_noise(splits[0], (TOKENS, D), 1.0, 6.0, ((0, 32), (1, 8)), (0, 1, 32, 2.75))
    cotangent = heavy_noise(splits[1], (TOKENS, D), 1.0, 6.0, ((0, 32), (1, 8)), (0, 1, 32, 2.75))
    up_weight = bell_draw(splits[2], (D, FF), D ** -0.5, 0.125, ((0, 32), (1, 8)))
    down_weight = bell_draw(splits[3], (FF, D), FF ** -0.5, 0.0625, ((0, 8), (1, 32)))
    return {"normed_input": normed_input, "cotangent": cotangent, "up_weight": up_weight, "down_weight": down_weight}


def reference(normed_input, cotangent, up_weight, down_weight):
    tokens = normed_input.shape[0]
    width = FF // FF_BLOCKS
    scale = lax.rsqrt(jnp.asarray(tokens, jnp.float32))

    def block(total, index):
        start = (index * width).astype(jnp.int32)
        up_block = lax.dynamic_slice_in_dim(up_weight, start, width, 1)
        down_block = lax.dynamic_slice_in_dim(down_weight, start, width, 0)
        pre = jnp.dot(normed_input, up_block, preferred_element_type=jnp.float32)
        rectified = jax.nn.relu(pre)
        act = (rectified * rectified).astype(jnp.bfloat16)
        act_grad = jnp.dot(cotangent, down_block.T, preferred_element_type=jnp.float32)
        pre_grad = (2.0 * rectified * act_grad).astype(jnp.bfloat16)
        down_part = jnp.dot(act.T, cotangent, preferred_element_type=jnp.float32) * scale
        up_part = jnp.dot(normed_input.T, pre_grad, preferred_element_type=jnp.float32) * scale
        partial_value = jnp.dot(pre_grad, up_block.T, preferred_element_type=jnp.float32).astype(jnp.bfloat16)
        partial_value = lax.optimization_barrier(partial_value)
        return (total + partial_value.astype(jnp.float32), (up_part, down_part))
    start_total = jnp.zeros(normed_input.shape, jnp.float32)
    total, parts = lax.scan(block, start_total, jnp.arange(FF_BLOCKS, dtype=jnp.int32))
    up_parts, down_parts = parts
    up_grad = jnp.moveaxis(up_parts, 0, 1).reshape(D, FF)
    down_grad = down_parts.reshape(FF, D)
    return (total.astype(jnp.bfloat16), up_grad, down_grad)
```

```python
import jax
import jax.numpy as jnp
from jax import lax
from jax.sharding import Mesh
from jax.sharding import PartitionSpec as P

BF = jnp.bfloat16
F32 = jnp.float32


def shift(value, axis, by):
    n = lax.axis_size(axis)
    return lax.ppermute(value, axis, [(i, (i + by) % n) for i in range(n)])


def gather4(own, axis):
    half = own.shape[0] // 2
    prev = shift(own, axis, 1)
    succ = shift(own, axis, -1)
    first = shift(prev[:half], axis, 1)
    second = shift(succ[half:], axis, -1)
    return [own, succ, jnp.concatenate([first, second], axis=0), prev]


def add(*terms):
    return sum(t.astype(F32) for t in terms).astype(BF)


def scatter4(terms, axis):
    half = terms[0].shape[0] // 2
    up = shift(terms[2][:half], axis, 1)
    down = shift(terms[2][half:], axis, -1)
    to_next = jnp.concatenate([add(terms[1][:half], up), terms[1][half:]], axis=0)
    to_prev = jnp.concatenate([terms[3][:half], add(terms[3][half:], down)], axis=0)
    return add(terms[0], shift(to_next, axis, 1), shift(to_prev, axis, -1))


def dot(left, right, lc, rc):
    return lax.dot_general(left, right, (((lc,), (rc,)), ((), ())), preferred_element_type=F32)


def per_device(normed_input, cotangent, up_weight, down_weight):
    z, x, c = lax.axis_index("z"), lax.axis_index("x"), lax.axis_index("c")
    nz = lax.axis_size("z")
    tokens = normed_input.shape[0] * nz * lax.axis_size("y")
    scale = lax.rsqrt(jnp.asarray(tokens, F32))

    both = jnp.stack([normed_input, cotangent])
    half = both.shape[1] // 2
    mine = lax.dynamic_slice_in_dim(both, c * half, half, 1)
    other = lax.dynamic_slice_in_dim(both, (1 - c) * half, half, 1)
    arrived = shift(other, "c", 1)
    ours = jnp.where(c == 0, jnp.concatenate([mine, arrived], 2), jnp.concatenate([arrived, mine], 2))
    xs, ks = ours[0], ours[1]

    pair = jnp.stack([up_weight, down_weight.T])
    rows, width = pair.shape[1], pair.shape[2] // 4
    quarters = jnp.moveaxis(pair.reshape(2, rows, 4, width), 2, 0)
    block = lax.all_to_all(quarters, "y", split_axis=0, concat_axis=0, tiled=True)
    block = jnp.moveaxis(block, 0, 1).reshape(2, 4 * rows, width)
    brows = 4 * rows

    def place(buf, value, offset):
        at = (z + offset - 2 * x) % nz * brows
        return lax.dynamic_update_slice(buf, value, (0, at, 0))

    whole = jnp.zeros((2, nz * brows, width), BF)
    whole = place(whole, block, 0)
    fwd, bwd = block, block
    for k in range(1, 4):
        fwd, bwd = shift(fwd, "z", 1), shift(bwd, "z", -1)
        whole = place(place(whole, fwd, -k), bwd, k)
    last = jnp.stack([shift(fwd[0], "z", 1), shift(bwd[1], "z", -1)])
    whole = place(whole, last, 4)
    partner = shift(whole, "c", 1)

    xt = jnp.concatenate(gather4(xs, "y"), axis=0)
    kt = jnp.concatenate(gather4(ks, "x"), axis=1)
    xw = jnp.concatenate(gather4(xt, "x"), axis=1)
    kw = jnp.concatenate(gather4(kt, "y"), axis=0)

    def grads(w):
        pre = dot(xw, w[0], 1, 0)
        rect = jax.nn.relu(pre)
        act = (rect * rect).astype(BF)
        pre_grad = (2.0 * rect * dot(kw, w[1], 1, 0)).astype(BF)
        return act, pre_grad

    act_p, pg_p = grads(partner)
    act_o, pg_o = grads(whole)
    partial = (dot(pg_o, whole[0], 1, 1) + dot(pg_p, partner[0], 1, 1)).astype(BF)

    def wgrads(act, pg):
        up = (dot(xw, pg, 0, 0) * scale).astype(BF)
        down = (dot(kw, act, 0, 0) * scale).astype(BF)
        return jnp.stack([up, down])

    sums = add(shift(wgrads(act_p, pg_p), "c", 1), wgrads(act_o, pg_o))

    def part(offset):
        at = (z + offset - 2 * x) % nz * brows
        return lax.dynamic_slice_in_dim(sums, at, brows, 1)

    far = part(4)
    fwd, bwd = shift(far[0], "z", 1), shift(far[1], "z", -1)
    ahead, behind = part(3), part(-3)
    fwd = jnp.stack([add(ahead[0], fwd), ahead[1]])
    bwd = jnp.stack([behind[0], add(behind[1], bwd)])
    for k in (2, 1):
        fwd, bwd = add(shift(fwd, "z", 1), part(k)), add(shift(bwd, "z", -1), part(-k))
    block = add(part(0), shift(fwd, "z", 1), shift(bwd, "z", -1))
    block = jnp.moveaxis(block.reshape(2, 4, rows, width), 1, 0)
    block = lax.all_to_all(block, "y", split_axis=0, concat_axis=0, tiled=True)
    block = jnp.moveaxis(block, 0, 2).reshape(2, rows, 4 * width).astype(F32)

    feats = partial.shape[1] // 8
    t = partial.shape[0] // 4
    low = [partial[:, (2 * j) * feats:(2 * j + 1) * feats] for j in range(4)]
    high = jnp.concatenate([partial[:, (2 * j + 1) * feats:(2 * j + 2) * feats] for j in range(4)], axis=1)
    low = scatter4(low, "x")
    low = scatter4([low[j * t:(j + 1) * t] for j in range(4)], "y")
    high = scatter4([high[j * t:(j + 1) * t] for j in range(4)], "y")
    high = scatter4([high[:, j * feats:(j + 1) * feats] for j in range(4)], "x")
    keep, give = jnp.where(c == 0, low, high), jnp.where(c == 0, high, low)
    got = shift(give, "c", 1)
    input_grad = jnp.where(c == 0, jnp.concatenate([keep, got], 0), jnp.concatenate([got, keep], 0))
    return input_grad, block[0], block[1].T


def solution(mesh):
    split = Mesh(mesh.devices.reshape(8, 4, 4, 2), ("z", "y", "x", "c"))
    fs, tp = ("z", "y"), ("x", "c")
    in_specs = (P(fs, tp), P(fs, tp), P(fs, tp), P(tp, fs))
    out_specs = (P(fs, tp), P(fs, tp), P(tp, fs))
    return jax.shard_map(
        per_device, mesh=split, in_specs=in_specs, out_specs=out_specs, check_vma=False
    )
```

```python
import jax
import jax.numpy as jnp
from jax import lax
from jax.sharding import Mesh
from jax.sharding import PartitionSpec as P

BF = jnp.bfloat16
F32 = jnp.float32


def shift(value, axis, by):
    n = lax.axis_size(axis)
    return lax.ppermute(value, axis, [(i, (i + by) % n) for i in range(n)])


def exchange(value, axes):
    return lax.all_to_all(value, axes, split_axis=0, concat_axis=0, tiled=True)


def gather4(own, axis, place):
    half = own.shape[0] // 2
    place(own, 0, 0)
    prev = shift(own, axis, 1)
    succ = shift(own, axis, -1)
    first = shift(prev[:half], axis, 1)
    second = shift(succ[half:], axis, -1)
    place(prev, 3, 0)
    place(succ, 1, 0)
    place(first, 2, 0)
    place(second, 2, half)


def add(*terms):
    return sum(t.astype(F32) for t in terms).astype(BF)


def dot(left, right, lc, rc):
    return lax.dot_general(left, right, (((lc,), (rc,)), ((), ())), preferred_element_type=F32)


def per_device(normed_input, cotangent, up_weight, down_weight):
    z, y, x, c = (lax.axis_index(a) for a in "zyxc")
    nz = lax.axis_size("z")
    tokens = normed_input.shape[0] * nz * lax.axis_size("y")
    scale = lax.rsqrt(jnp.asarray(tokens, F32))
    t, f = normed_input.shape[0] // 2, normed_input.shape[1]

    rows, width = up_weight.shape[0], up_weight.shape[1] // 4
    pair = jnp.stack([up_weight, down_weight.T])
    quarters = jnp.moveaxis(pair.reshape(2, rows, 4, width), 2, 0)
    block = jnp.moveaxis(exchange(quarters, "y"), 0, 1).reshape(2, 4 * rows, width)
    brows = 4 * rows

    def spread(value):
        return jnp.broadcast_to(value.reshape(1, 2, t, f), (4, 2, t, f)).reshape(8, t, f)

    kt = exchange(spread(cotangent), ("y", "c")).reshape(4, 2, t, f)
    kt = jnp.moveaxis(kt, 1, 2).reshape(4 * t, 2 * f)
    xt = jnp.moveaxis(exchange(spread(normed_input), ("x", "c")), 0, 1).reshape(t, 8 * f)

    def at(which, offset):
        first = 2 * x if which else 0
        return (z + offset - first) % nz * brows

    whole = [jnp.zeros((nz * brows, width), BF)] * 2

    def place(value, offset):
        for i in range(2):
            whole[i] = lax.dynamic_update_slice(whole[i], value[i], (at(i, offset), 0))

    place(block, 0)
    fwd, bwd = block, block
    for k in range(1, 4):
        fwd, bwd = shift(fwd, "z", 1), shift(bwd, "z", -1)
        place(fwd, -k)
        place(bwd, k)
    place([shift(fwd[0], "z", 1), shift(bwd[1], "z", -1)], 4)
    partner = shift(jnp.stack(whole), "c", 1)

    kw = [jnp.zeros((4 * t, 8 * f), BF)]
    xw = [jnp.zeros((4 * t, 8 * f), BF)]

    def place_k(value, far, half):
        kw[0] = lax.dynamic_update_slice(kw[0], value, (half, far * 2 * f))

    def place_x(value, far, half):
        xw[0] = lax.dynamic_update_slice(xw[0], value, ((y + far) % 4 * t + half, 0))

    gather4(kt, "x", place_k)
    gather4(xt, "y", place_x)
    kw, xw = kw[0], xw[0]

    def grads(up, down):
        rect = jax.nn.relu(dot(xw, up, 1, 0))
        act = (rect * rect).astype(BF)
        pre_grad = (2.0 * rect * dot(kw, down, 1, 0)).astype(BF)
        return act, pre_grad

    def wgrads(act, pg):
        up = (dot(xw, pg, 0, 0) * scale).astype(BF)
        down = (dot(kw, act, 0, 0) * scale).astype(BF)
        return jnp.stack([up, down])

    act_p, pg_p = grads(partner[0], partner[1])
    theirs = shift(wgrads(act_p, pg_p), "c", 1)
    act_o, pg_o = grads(whole[0], whole[1])
    sums = add(theirs, wgrads(act_o, pg_o))
    partial = (dot(pg_o, whole[0], 1, 1) + dot(pg_p, partner[0], 1, 1)).astype(BF)

    partial = partial.reshape(4, 2, t // 2, 8, f)
    low = jnp.moveaxis(partial[:, 0].reshape(2 * t, 8, f), 1, 0)
    low = exchange(low, ("x", "c")).reshape(4, 2, 4, t // 2, f).astype(F32).sum(0).astype(BF)
    low = exchange(jnp.moveaxis(low, 1, 0), "y").astype(F32).sum(0).astype(BF)
    high = exchange(partial[:, 1].reshape(4, t // 2, 8 * f), "y").astype(F32).sum(0).astype(BF)
    high = jnp.moveaxis(high.reshape(t // 2, 8, f), 1, 0)
    high = exchange(high, ("x", "c")).reshape(4, 2, t // 2, f).astype(F32).sum(0).astype(BF)
    input_grad = jnp.stack([low, high], 1).reshape(2 * t, f)

    def part(which, offset):
        return lax.dynamic_slice_in_dim(sums[which], at(which, offset), brows, 0)

    def both(offset):
        return jnp.stack([part(0, offset), part(1, offset)])

    fwd, bwd = shift(part(0, 4), "z", 1), shift(part(1, 4), "z", -1)
    fwd = jnp.stack([add(part(0, 3), fwd), part(1, 3)])
    bwd = jnp.stack([part(0, -3), add(part(1, -3), bwd)])
    for k in (2, 1):
        fwd, bwd = add(shift(fwd, "z", 1), both(k)), add(shift(bwd, "z", -1), both(-k))
    block = add(both(0), shift(fwd, "z", 1), shift(bwd, "z", -1))
    block = exchange(jnp.moveaxis(block.reshape(2, 4, rows, width), 1, 0), "y")
    block = jnp.moveaxis(block, 0, 2).reshape(2, rows, 4 * width).astype(F32)
    return input_grad, block[0], block[1].T


def solution(mesh):
    split = Mesh(mesh.devices.reshape(8, 4, 4, 2), ("z", "y", "x", "c"))
    fs, tp = ("z", "y"), ("x", "c")
    in_specs = (P(fs, tp), P(fs, tp), P(fs, tp), P(tp, fs))
    out_specs = (P(fs, tp), P(fs, tp), P(tp, fs))
    return jax.shard_map(
        per_device, mesh=split, in_specs=in_specs, out_specs=out_specs, check_vma=False
    )
```

```python
import jax
import jax.numpy as jnp
from jax import lax
from jax.sharding import Mesh
from jax.sharding import PartitionSpec as P

BF = jnp.bfloat16
F32 = jnp.float32


def shift(value, axis, by):
    n = lax.axis_size(axis)
    return lax.ppermute(value, axis, [(i, (i + by) % n) for i in range(n)])


def ring(value, by, x_core):
    ny, nx = lax.axis_size("y"), lax.axis_size("x")
    pairs = []
    for y in range(ny):
        for x in range(nx):
            for c in range(2):
                to = (y, (x + by) % nx) if c == x_core else ((y + by) % ny, x)
                pairs.append(((y * nx + x) * 2 + c, (to[0] * nx + to[1]) * 2 + c))
    return lax.ppermute(value, ("y", "x", "c"), pairs)


def exchange(value, axes):
    return lax.all_to_all(value, axes, split_axis=0, concat_axis=0, tiled=True)


def add(*terms):
    return sum(t.astype(F32) for t in terms).astype(BF)


def put(buf, value, *start):
    return lax.dynamic_update_slice(buf, value, start)


def dot(left, right, lc, rc):
    return lax.dot_general(left, right, (((lc,), (rc,)), ((), ())), preferred_element_type=F32)


def scatter4(terms, x_core):
    up = ring(terms[2][0], 1, x_core)
    down = ring(terms[2][1], -1, x_core)
    to_next = jnp.stack([add(terms[1][0], up), terms[1][1]])
    to_prev = jnp.stack([terms[3][0], add(terms[3][1], down)])
    a, b = ring(to_next, 1, x_core), ring(to_prev, -1, x_core)
    return [add(terms[0][i], a[i], b[i]) for i in range(2)]


def per_device(normed_input, cotangent, up_weight, down_weight):
    z, x, c = (lax.axis_index(a) for a in "zxc")
    nz = lax.axis_size("z")
    tokens = normed_input.shape[0] * nz * lax.axis_size("y")
    scale = lax.rsqrt(jnp.asarray(tokens, F32))
    t, f = normed_input.shape[0] // 2, normed_input.shape[1]
    first = c == 0

    swap = shift(jnp.where(first, cotangent, normed_input), "c", 1)

    rows, width = up_weight.shape[0], up_weight.shape[1] // 4
    pair = jnp.stack([up_weight, down_weight.T])
    quarters = jnp.moveaxis(pair.reshape(2, rows, 4, width), 2, 0)
    block = jnp.moveaxis(exchange(quarters, "y"), 0, 1).reshape(2, 4 * rows, width)
    brows = 4 * rows

    mine = jnp.concatenate(
        [jnp.where(first, normed_input, swap), jnp.where(first, swap, cotangent)], 1
    ).reshape(2, t, 2 * f)
    mine = jnp.where(first, mine, mine[::-1])
    prev, succ = ring(mine, 1, 1), ring(mine, -1, 1)
    stage = jnp.zeros((2, 4, t, 2 * f), BF)
    stage = put(stage, mine[:, None], 0, 0, 0, 0)
    far = ring(prev[0], 1, 1), ring(succ[1], -1, 1)
    stage = put(stage, prev[:, None], 0, 3, 0, 0)
    stage = put(stage, succ[:, None], 0, 1, 0, 0)
    stage = put(stage, far[0][None, None], 0, 2, 0, 0)
    stage = put(stage, far[1][None, None], 1, 2, 0, 0)
    prev, succ = ring(stage, 1, 0), ring(stage, -1, 0)
    far = ring(prev[0], 1, 0), ring(succ[1], -1, 0)
    sides = shift(jnp.stack([succ[1], prev[1]]), "c", 1)
    chunks = [
        (stage[0], shift(stage[1], "c", 1)),
        (succ[0], sides[0]),
        (far[0], shift(far[1], "c", 1)),
        (prev[0], sides[1]),
    ]
    xw = jnp.zeros((4 * t, 8 * f), BF)
    kw = jnp.zeros((4 * t, 8 * f), BF)
    for j in (0, 1, 3, 2):
        own, other = chunks[j]
        xw = put(xw, jnp.where(first, own, other).reshape(4 * t, 2 * f), 0, 2 * f * j)
        kb = jnp.moveaxis(jnp.where(first, other, own), 0, 1).reshape(t, 8 * f)
        kw = put(kw, kb, t * j, 0)

    def at(offset):
        return (z + offset - 2 * x) % nz * brows

    def place(buf, value, offset):
        return put(buf, value, 0, at(offset), 0)

    whole = jnp.zeros((2, nz * brows, width), BF)
    whole = place(whole, block, 0)
    fwd, bwd = block, block
    for k in range(1, 4):
        fwd, bwd = shift(fwd, "z", 1), shift(bwd, "z", -1)
        whole = place(place(whole, fwd, -k), bwd, k)
    whole = place(whole, jnp.stack([shift(fwd[0], "z", 1), shift(bwd[1], "z", -1)]), 4)
    partner = shift(whole, "c", 1)
    weights = jnp.zeros((2, nz * brows, 2 * width), BF)
    weights = put(put(weights, whole, 0, 0, 0), partner, 0, 0, width)
    up, down = weights[0], weights[1]

    rect = jax.nn.relu(dot(xw, up, 1, 0))
    act = (rect * rect).astype(BF)
    pre_grad = (2.0 * rect * dot(kw, down, 1, 0)).astype(BF)
    down_part = (dot(kw, act, 0, 0) * scale).astype(BF)
    up_part = (dot(xw, pre_grad, 0, 0) * scale).astype(BF)
    theirs = shift(jnp.stack([up_part[:, width:], down_part[:, width:]]), "c", 1)
    sums = [add(up_part[:, :width], theirs[0]), add(down_part[:, :width], theirs[1])]
    partial = dot(pre_grad, up, 1, 1).astype(BF).reshape(4, t, 4, 2, f)

    def part(i, offset):
        return lax.dynamic_slice_in_dim(sums[i], at(offset), brows, 0)

    def both(offset):
        return jnp.stack([part(0, offset), part(1, offset)])

    fwd, bwd = shift(part(0, 4), "z", 1), shift(part(1, 4), "z", -1)
    fwd = jnp.stack([add(part(0, 3), fwd), part(1, 3)])
    bwd = jnp.stack([part(0, -3), add(part(1, -3), bwd)])
    for k in (2, 1):
        fwd, bwd = add(shift(fwd, "z", 1), both(k)), add(shift(bwd, "z", -1), both(-k))
    block = add(both(0), shift(fwd, "z", 1), shift(bwd, "z", -1))
    block = exchange(jnp.moveaxis(block.reshape(2, 4, rows, width), 1, 0), "y")
    block = jnp.moveaxis(block, 0, 2).reshape(2, rows, 4 * width).astype(F32)

    low = jnp.moveaxis(partial[:, :, :, 0], 2, 0)
    high = jnp.moveaxis(partial[:, :, :, 1], 2, 1)
    keep, give = jnp.where(first, low, high), jnp.where(first, high, low)
    got = shift(give, "c", 1)
    mine = scatter4([(keep[j], got[j]) for j in range(4)], 0)
    mine = scatter4([(mine[0][j], mine[1][j]) for j in range(4)], 1)
    input_grad = jnp.concatenate([jnp.where(first, mine[0], mine[1]), jnp.where(first, mine[1], mine[0])], 0)
    return input_grad, block[0], block[1].T


def solution(mesh):
    split = Mesh(mesh.devices.reshape(8, 4, 4, 2), ("z", "y", "x", "c"))
    fs, tp = ("z", "y"), ("x", "c")
    in_specs = (P(fs, tp), P(fs, tp), P(fs, tp), P(tp, fs))
    out_specs = (P(fs, tp), P(fs, tp), P(tp, fs))
    return jax.shard_map(
        per_device, mesh=split, in_specs=in_specs, out_specs=out_specs, check_vma=False
    )
```

```python
import functools

import jax
import jax.numpy as jnp
from jax import lax
from jax.experimental import pallas as pl
from jax.experimental.pallas import tpu as pltpu
from jax.sharding import Mesh
from jax.sharding import PartitionSpec as P


BF = jnp.bfloat16
F32 = jnp.float32


def shift(value, axis, by):
    n = lax.axis_size(axis)
    return lax.ppermute(value, axis, [(i, (i + by) % n) for i in range(n)])


def ring(value, by, x_core):
    ny, nx = lax.axis_size("y"), lax.axis_size("x")
    pairs = []
    for y in range(ny):
        for x in range(nx):
            for c in range(2):
                to = (y, (x + by) % nx) if c == x_core else ((y + by) % ny, x)
                pairs.append(((y * nx + x) * 2 + c, (to[0] * nx + to[1]) * 2 + c))
    return lax.ppermute(value, ("y", "x", "c"), pairs)


def exchange(value, axes):
    return lax.all_to_all(value, axes, split_axis=0, concat_axis=0, tiled=True)


def add(*terms):
    return sum(t.astype(F32) for t in terms).astype(BF)


def put(buf, value, *start):
    return lax.dynamic_update_slice(buf, value, start)


def dot(left, right, lc, rc):
    return lax.dot_general(left, right, (((lc,), (rc,)), ((), ())), preferred_element_type=F32)


def scatter4(terms, x_core):
    up = ring(terms[2][0], 1, x_core)
    down = ring(terms[2][1], -1, x_core)
    to_next = jnp.stack([add(terms[1][0], up), terms[1][1]])
    to_prev = jnp.stack([terms[3][0], add(terms[3][1], down)])
    a = ring(to_next, 1, x_core)
    b = ring(to_prev, -1, x_core)
    return [add(terms[0][i], a[i], b[i]) for i in range(2)]


def grads_kernel(core, stage, succ, far, prev, theirs, their_far, own_w, other_w,
                 give, keep, pre_grad, xw, kw, ww, rect, act, pg, gives, keeps, sems, outs, *, scale):
    blocks, t, _ = xw.shape
    f, w = kw.shape[2], own_w.shape[2]
    is_first = core[0] == 0
    pairs = ((stage.at[0], theirs.at[0]), (succ.at[0], theirs.at[1]), (far, their_far), (prev.at[0], theirs.at[2]))

    def weights(n):
        return [
            pltpu.make_async_copy(v.at[n], ww.at[n, :, pl.ds(k * w, w)], sems.at[2 * n + k])
            for k, v in enumerate((own_w, other_w))
        ]

    def tokens(core_0, which):
        for j, (mine, other) in enumerate(pairs):
            if which == 0:
                source, target = mine if core_0 else other, xw.at[:, :, pl.ds(j * f, f)]
            else:
                source, target = other if core_0 else mine, kw.at[:, pl.ds(j * t, t)]
            yield pltpu.make_async_copy(source, target, sems.at[4 + 4 * which + j])

    def start(core_0):
        for n in range(2):
            for copy in [*weights(n), *tokens(core_0, n)]:
                copy.start()

    @pl.when(is_first)
    def _():
        start(True)

    @pl.when(jnp.logical_not(is_first))
    def _():
        start(False)

    for copy in [*weights(0), *tokens(True, 0)]:
        copy.wait()

    def forward(i, carry):
        rect[i] = jnp.maximum(dot(xw[i], ww[0], 1, 0), 0.0)
        return carry

    lax.fori_loop(0, blocks, forward, 0)
    for copy in [*weights(1), *tokens(True, 1)]:
        copy.wait()

    def backward(i, carry):
        rows = pl.ds(i * t, t)
        ag = dot(kw[0, rows], ww[1, 0:f], 1, 0)
        for q in range(1, blocks):
            ag += dot(kw[q, rows], ww[1, q * f:(q + 1) * f], 1, 0)
        act[rows] = (rect[i] * rect[i]).astype(BF)
        pg[rows] = (2.0 * rect[i] * ag).astype(BF)
        return carry

    lax.fori_loop(0, blocks, backward, 0)
    copies = [pltpu.make_async_copy(pg, pre_grad, outs.at[0])]
    copies[0].start()

    def results(q, r):
        at = (slice(None), pl.ds(pl.multiple_of(q * f + r * w, w), w))
        pairs = ((gives, give), (keeps, keep))
        return [
            pltpu.make_async_copy(source.at[at], target.at[at], outs.at[1 + 2 * (q * (f // w) + r) + k])
            for k, (source, target) in enumerate(pairs)
        ]

    def features(q, carry):
        for r in range(f // w):
            cols = pl.ds(pl.multiple_of(q * f + r * w, w), w)
            up = dot(xw[:, :, cols].reshape(blocks * t, w), pg[...], 0, 0)
            down = dot(kw[q, :, r * w:(r + 1) * w], act[...], 0, 0)
            for n, part in enumerate((up, down)):
                part = (part * scale).astype(BF)
                keeps[n, cols], gives[n, cols] = part[:, :w], part[:, w:]
            for copy in results(q, r):
                copy.start()
        return carry

    lax.fori_loop(0, blocks, features, 0)
    for q in range(blocks):
        for r in range(f // w):
            copies += results(q, r)
    for copy in copies:
        copy.wait()


def input_kernel(core, pre_grad, own_w, other_w, keep, give, pg, uw, low, high, sems, outs):
    t, f = low.shape[2], low.shape[3]
    w = own_w.shape[2]
    is_first = core[0] == 0
    copies = [
        pltpu.make_async_copy(pre_grad, pg, sems.at[0]),
        pltpu.make_async_copy(own_w.at[0], uw.at[:, pl.ds(0, w)], sems.at[1]),
        pltpu.make_async_copy(other_w.at[0], uw.at[:, pl.ds(w, w)], sems.at[2]),
    ]
    for copy in copies:
        copy.start()
    for copy in copies:
        copy.wait()

    def results(j, core_0):
        a, b = (keep, give) if core_0 else (give, keep)
        return [
            pltpu.make_async_copy(low.at[j], a.at[j], outs.at[2 * j]),
            pltpu.make_async_copy(high.at[:, j], b.at[:, j], outs.at[2 * j + 1]),
        ]

    def features(j, carry):
        for k in range(2):
            right = uw[pl.ds((2 * j + k) * f, f)]
            for i in range(4):
                part = dot(pg[i * t:(i + 1) * t], right, 1, 1).astype(BF)
                if k == 0:
                    low[j, i] = part
                else:
                    high[i, j] = part

        @pl.when(is_first)
        def _():
            for copy in results(j, True):
                copy.start()

        @pl.when(jnp.logical_not(is_first))
        def _():
            for copy in results(j, False):
                copy.start()

        return carry

    lax.fori_loop(0, 4, features, 0)
    for j in range(4):
        for copy in results(j, True):
            copy.wait()


SMEM = pl.BlockSpec(memory_space=pltpu.SMEM)
HBM = pl.BlockSpec(memory_space=pltpu.HBM)
DMA = pltpu.SemaphoreType.DMA


def per_device(normed_input, cotangent, up_weight, down_weight):
    z, _, x, c = (lax.axis_index(a) for a in "zyxc")
    nz = lax.axis_size("z")
    tokens = normed_input.shape[0] * nz * lax.axis_size("y")
    scale = tokens ** -0.5
    t, f = normed_input.shape[0] // 2, normed_input.shape[1]
    first = c == 0
    core = c.reshape(1).astype(jnp.int32)

    swap = shift(jnp.where(first, cotangent, normed_input), "c", 1)

    rows, width = up_weight.shape[0], up_weight.shape[1] // 4
    pair = jnp.stack([up_weight, down_weight.T])
    quarters = jnp.moveaxis(pair.reshape(2, rows, 4, width), 2, 0)
    block = jnp.moveaxis(exchange(quarters, "y"), 0, 1).reshape(2, 4 * rows, width)
    brows = 4 * rows

    mine = jnp.concatenate(
        [jnp.where(first, normed_input, swap), jnp.where(first, swap, cotangent)], 1
    ).reshape(2, t, 2 * f)
    mine = jnp.where(first, mine, mine[::-1])
    prev, succ = ring(mine, 1, 1), ring(mine, -1, 1)
    stage = jnp.zeros((2, 4, t, 2 * f), BF)
    stage = put(stage, mine[:, None], 0, 0, 0, 0)
    far = ring(prev[0], 1, 1), ring(succ[1], -1, 1)
    stage = put(stage, prev[:, None], 0, 3, 0, 0)
    stage = put(stage, succ[:, None], 0, 1, 0, 0)
    stage = put(stage, far[0][None, None], 0, 2, 0, 0)
    stage = put(stage, far[1][None, None], 1, 2, 0, 0)
    prev, succ = ring(stage, 1, 0), ring(stage, -1, 0)
    far = ring(prev[0], 1, 0), ring(succ[1], -1, 0)
    theirs = shift(jnp.stack([stage[1], succ[1], prev[1]]), "c", 1)
    their_far = shift(far[1], "c", 1)

    def at(offset):
        return (z + offset - 2 * x) % nz * brows

    def place(buf, value, offset):
        return put(buf, value, 0, at(offset), 0)

    whole = jnp.zeros((2, nz * brows, width), BF)
    whole = place(whole, block, 0)
    fwd, bwd = block, block
    for k in range(1, 4):
        fwd, bwd = shift(fwd, "z", 1), shift(bwd, "z", -1)
        whole = place(place(whole, fwd, -k), bwd, k)
    whole = place(whole, shift(fwd, "z", 1), 4)
    partner = shift(whole, "c", 1)

    d = nz * brows
    half = jax.ShapeDtypeStruct((2, d, width), BF)
    give, keep, pre_grad = pl.pallas_call(
        functools.partial(grads_kernel, scale=scale),
        out_shape=(half, half, jax.ShapeDtypeStruct((4 * t, 2 * width), BF)),
        in_specs=[SMEM] + [HBM] * 8,
        out_specs=(HBM,) * 3,
        scratch_shapes=[
            pltpu.VMEM((4, t, d), BF),
            pltpu.VMEM((4, 4 * t, 2 * f), BF),
            pltpu.VMEM((2, d, 2 * width), BF),
            pltpu.VMEM((4, t, 2 * width), F32),
            pltpu.VMEM((4 * t, 2 * width), BF),
            pltpu.VMEM((4 * t, 2 * width), BF),
            pltpu.VMEM((2, d, width), BF),
            pltpu.VMEM((2, d, width), BF),
            DMA((12,)),
            DMA((1 + 2 * (d // width),)),
        ],
        cost_estimate=pl.CostEstimate(flops=2 * 4 * 4 * t * d * 2 * width, bytes_accessed=1 << 24, transcendentals=0),
        name="grads",
    )(core, stage, succ, far[0], prev, theirs, their_far, whole, partner)
    got_w = shift(give, "c", 1)

    blocks = jax.ShapeDtypeStruct((4, 4, t, f), BF)
    keep_i, give_i = pl.pallas_call(
        input_kernel,
        out_shape=(blocks, blocks),
        in_specs=[SMEM] + [HBM] * 3,
        out_specs=(HBM,) * 2,
        scratch_shapes=[
            pltpu.VMEM((4 * t, 2 * width), BF),
            pltpu.VMEM((d, 2 * width), BF),
            pltpu.VMEM((4, 4, t, f), BF),
            pltpu.VMEM((4, 4, t, f), BF),
            DMA((3,)),
            DMA((8,)),
        ],
        cost_estimate=pl.CostEstimate(flops=2 * 4 * t * d * 2 * width, bytes_accessed=1 << 23, transcendentals=0),
        name="input",
    )(core, pre_grad, whole, partner)
    got_i = shift(give_i, "c", 1)

    def part(offset):
        start = (0, at(offset), 0)
        return [lax.dynamic_slice(v, start, (2, brows, width)) for v in (keep, got_w)]

    fwd = shift(add(*part(4)), "z", 1)
    fwd, bwd = shift(add(fwd, *part(3)), "z", 1), shift(add(*part(-3)), "z", -1)
    fwd, bwd = shift(add(fwd, *part(2)), "z", 1), shift(add(bwd, *part(-2)), "z", -1)
    fwd, bwd = shift(add(fwd, *part(1)), "z", 1), shift(add(bwd, *part(-1)), "z", -1)
    block = add(fwd, bwd, *part(0))
    block = exchange(jnp.moveaxis(block.reshape(2, 4, rows, width), 1, 0), "y")
    block = jnp.moveaxis(block, 0, 2).reshape(2, rows, 4 * width).astype(F32)

    mine = scatter4([(keep_i[j], got_i[j]) for j in range(4)], 0)
    mine = [jnp.stack([mine[0][j], mine[1][j]]) for j in range(4)]
    mine = add(mine[0], *(ring(mine[j], j if j < 3 else -1, 1) for j in (2, 1, 3)))
    input_grad = jnp.concatenate([jnp.where(first, mine[0], mine[1]), jnp.where(first, mine[1], mine[0])], 0)
    return input_grad, block[0], block[1].T


def solution(mesh):
    split = Mesh(mesh.devices.reshape(8, 4, 4, 2), ("z", "y", "x", "c"))
    fs, tp = ("z", "y"), ("x", "c")
    in_specs = (P(fs, tp), P(fs, tp), P(fs, tp), P(tp, fs))
    out_specs = (P(fs, tp), P(fs, tp), P(tp, fs))

    return jax.shard_map(per_device, mesh=split, in_specs=in_specs, out_specs=out_specs, check_vma=False)
```

```python
import functools

import jax
import jax.numpy as jnp
from jax import lax
from jax.experimental import pallas as pl
from jax.experimental.pallas import tpu as pltpu
from jax.sharding import Mesh
from jax.sharding import PartitionSpec as P


BF = jnp.bfloat16
F32 = jnp.float32


def shift(value, axis, by):
    n = lax.axis_size(axis)
    return lax.ppermute(value, axis, [(i, (i + by) % n) for i in range(n)])


def ring(value, by, x_core, cross=False):
    ny, nx = lax.axis_size("y"), lax.axis_size("x")
    pairs = []
    for y in range(ny):
        for x in range(nx):
            for c in range(2):
                to = (y, (x + by) % nx) if c == x_core else ((y + by) % ny, x)
                pairs.append(((y * nx + x) * 2 + c, (to[0] * nx + to[1]) * 2 + (1 - c if cross else c)))
    return lax.ppermute(value, ("y", "x", "c"), pairs)


def exchange(value, axes):
    return lax.all_to_all(value, axes, split_axis=0, concat_axis=0, tiled=True)


def add(*terms):
    return sum(t.astype(F32) for t in terms).astype(BF)


def put(buf, value, *start):
    return lax.dynamic_update_slice(buf, value, start)


def dot(left, right, lc, rc):
    return lax.dot_general(left, right, (((lc,), (rc,)), ((), ())), preferred_element_type=F32)


def scatter4(terms, x_core):
    up = ring(terms[2][0], 1, x_core)
    down = ring(terms[2][1], -1, x_core)
    to_next = jnp.stack([add(terms[1][0], up), terms[1][1]])
    to_prev = jnp.stack([terms[3][0], add(terms[3][1], down)])
    a = ring(to_next, 1, x_core)
    b = ring(to_prev, -1, x_core)
    return [add(terms[0][i], a[i], b[i]) for i in range(2)]


def grads_kernel(core, stage, succ, far, prev, theirs, their_far, own_w, other_w,
                 give, keep, pre_grad, xw, kw, ww, rect, act, pg, gives, keeps, sems, outs, *, scale):
    blocks, t, _ = xw.shape
    f, w = kw.shape[2], own_w.shape[2]
    is_first = core[0] == 0
    pairs = ((stage.at[0], theirs.at[0]), (succ.at[0], theirs.at[1]), (far, their_far), (prev.at[0], theirs.at[2]))

    def weights(n):
        return [
            pltpu.make_async_copy(v.at[n], ww.at[n, :, pl.ds(k * w, w)], sems.at[2 * n + k])
            for k, v in enumerate((own_w, other_w))
        ]

    def tokens(core_0, which):
        for j, (mine, other) in enumerate(pairs):
            if which == 0:
                source, target = mine if core_0 else other, xw.at[:, :, pl.ds(j * f, f)]
            else:
                source, target = other if core_0 else mine, kw.at[:, pl.ds(j * t, t)]
            yield pltpu.make_async_copy(source, target, sems.at[4 + 4 * which + j])

    def start(core_0):
        for n in range(2):
            for copy in [*weights(n), *tokens(core_0, n)]:
                copy.start()

    @pl.when(is_first)
    def _():
        start(True)

    @pl.when(jnp.logical_not(is_first))
    def _():
        start(False)

    for copy in [*weights(0), *tokens(True, 0)]:
        copy.wait()

    def forward(i, carry):
        rect[i] = jnp.maximum(dot(xw[i], ww[0], 1, 0), 0.0)
        return carry

    lax.fori_loop(0, blocks, forward, 0)
    for copy in [*weights(1), *tokens(True, 1)]:
        copy.wait()

    def backward(i, carry):
        rows = pl.ds(i * t, t)
        ag = dot(kw[0, rows], ww[1, 0:f], 1, 0)
        for q in range(1, blocks):
            ag += dot(kw[q, rows], ww[1, q * f:(q + 1) * f], 1, 0)
        act[rows] = (rect[i] * rect[i]).astype(BF)
        pg[rows] = (2.0 * rect[i] * ag).astype(BF)
        return carry

    lax.fori_loop(0, blocks, backward, 0)
    copies = [pltpu.make_async_copy(pg, pre_grad, outs.at[0])]
    copies[0].start()

    def results(q, r):
        at = (slice(None), pl.ds(pl.multiple_of(q * f + r * w, w), w))
        pairs = ((gives, give), (keeps, keep))
        return [
            pltpu.make_async_copy(source.at[at], target.at[at], outs.at[1 + 2 * (q * (f // w) + r) + k])
            for k, (source, target) in enumerate(pairs)
        ]

    def features(q, carry):
        for r in range(f // w):
            cols = pl.ds(pl.multiple_of(q * f + r * w, w), w)
            up = dot(xw[:, :, cols].reshape(blocks * t, w), pg[...], 0, 0)
            down = dot(kw[q, :, r * w:(r + 1) * w], act[...], 0, 0)
            for n, part in enumerate((up, down)):
                part = (part * scale).astype(BF)
                keeps[n, cols], gives[n, cols] = part[:, :w], part[:, w:]
            for copy in results(q, r):
                copy.start()
        return carry

    lax.fori_loop(0, blocks, features, 0)
    for q in range(blocks):
        for r in range(f // w):
            copies += results(q, r)
    for copy in copies:
        copy.wait()


def input_kernel(core, pre_grad, own_w, other_w, keep, give, pg, uw, low, high, sems, outs):
    t, f = low.shape[2], low.shape[3]
    w = own_w.shape[2]
    is_first = core[0] == 0
    copies = [
        pltpu.make_async_copy(pre_grad, pg, sems.at[0]),
        pltpu.make_async_copy(own_w.at[0], uw.at[:, pl.ds(0, w)], sems.at[1]),
        pltpu.make_async_copy(other_w.at[0], uw.at[:, pl.ds(w, w)], sems.at[2]),
    ]
    for copy in copies:
        copy.start()
    for copy in copies:
        copy.wait()

    def results(j, core_0):
        a, b = (keep, give) if core_0 else (give, keep)
        return [
            pltpu.make_async_copy(low.at[j], a.at[j], outs.at[2 * j]),
            pltpu.make_async_copy(high.at[:, j], b.at[:, j], outs.at[2 * j + 1]),
        ]

    def features(j, carry):
        for k in range(2):
            right = uw[pl.ds((2 * j + k) * f, f)]
            for i in range(4):
                part = dot(pg[i * t:(i + 1) * t], right, 1, 1).astype(BF)
                if k == 0:
                    low[j, i] = part
                else:
                    high[i, j] = part

        @pl.when(is_first)
        def _():
            for copy in results(j, True):
                copy.start()

        @pl.when(jnp.logical_not(is_first))
        def _():
            for copy in results(j, False):
                copy.start()

        return carry

    lax.fori_loop(0, 4, features, 0)
    for j in range(4):
        for copy in results(j, True):
            copy.wait()


SMEM = pl.BlockSpec(memory_space=pltpu.SMEM)
HBM = pl.BlockSpec(memory_space=pltpu.HBM)
DMA = pltpu.SemaphoreType.DMA


def per_device(normed_input, cotangent, up_weight, down_weight):
    z, _, x, c = (lax.axis_index(a) for a in "zyxc")
    nz = lax.axis_size("z")
    tokens = normed_input.shape[0] * nz * lax.axis_size("y")
    scale = tokens ** -0.5
    t, f = normed_input.shape[0] // 2, normed_input.shape[1]
    first = c == 0
    core = c.reshape(1).astype(jnp.int32)

    swap = shift(jnp.where(first, cotangent, normed_input), "c", 1)

    rows, width = up_weight.shape[0], up_weight.shape[1] // 4
    pair = jnp.stack([up_weight, down_weight.T])
    quarters = jnp.moveaxis(pair.reshape(2, rows, 4, width), 2, 0)
    block = jnp.moveaxis(exchange(quarters, "y"), 0, 1).reshape(2, 4 * rows, width)
    brows = 4 * rows

    mine = jnp.concatenate(
        [jnp.where(first, normed_input, swap), jnp.where(first, swap, cotangent)], 1
    ).reshape(2, t, 2 * f)
    mine = jnp.where(first, mine, mine[::-1])
    prev, succ = ring(mine, 1, 1), ring(mine, -1, 1)
    stage = jnp.zeros((2, 4, t, 2 * f), BF)
    stage = put(stage, mine[:, None], 0, 0, 0, 0)
    far = prev[0], succ[1]
    far = ring(far[0], 1, 1), ring(far[1], -1, 1)
    stage = put(stage, prev[:, None], 0, 3, 0, 0)
    stage = put(stage, succ[:, None], 0, 1, 0, 0)
    stage = put(stage, far[0][None, None], 0, 2, 0, 0)
    stage = put(stage, far[1][None, None], 1, 2, 0, 0)
    prev, succ = ring(stage, 1, 0), ring(stage, -1, 0)
    far, their_far = ring(prev[0], 1, 0), ring(succ[1], -1, 0, cross=True)
    theirs = shift(jnp.stack([stage[1], succ[1], prev[1]]), "c", 1)

    def at(offset):
        return (z + offset - 2 * x) % nz * brows

    def place(buf, value, offset):
        return put(buf, value, 0, at(offset), 0)

    whole = jnp.zeros((2, nz * brows, width), BF)
    whole = place(whole, block, 0)
    fwd, bwd = block, block
    for k in range(1, 4):
        fwd, bwd = shift(fwd, "z", 1), shift(bwd, "z", -1)
        whole = place(place(whole, fwd, -k), bwd, k)
    whole = place(whole, shift(fwd, "z", 1), 4)
    partner = shift(whole, "c", 1)

    d = nz * brows
    half = jax.ShapeDtypeStruct((2, d, width), BF)
    give, keep, pre_grad = pl.pallas_call(
        functools.partial(grads_kernel, scale=scale),
        out_shape=(half, half, jax.ShapeDtypeStruct((4 * t, 2 * width), BF)),
        in_specs=[SMEM] + [HBM] * 8,
        out_specs=(HBM,) * 3,
        scratch_shapes=[
            pltpu.VMEM((4, t, d), BF),
            pltpu.VMEM((4, 4 * t, 2 * f), BF),
            pltpu.VMEM((2, d, 2 * width), BF),
            pltpu.VMEM((4, t, 2 * width), F32),
            pltpu.VMEM((4 * t, 2 * width), BF),
            pltpu.VMEM((4 * t, 2 * width), BF),
            pltpu.VMEM((2, d, width), BF),
            pltpu.VMEM((2, d, width), BF),
            DMA((12,)),
            DMA((1 + 2 * (d // width),)),
        ],
        cost_estimate=pl.CostEstimate(flops=2 * 4 * 4 * t * d * 2 * width, bytes_accessed=1 << 24, transcendentals=0),
        name="grads",
    )(core, stage, succ, far, prev, theirs, their_far, whole, partner)
    got_w = shift(give, "c", 1)

    blocks = jax.ShapeDtypeStruct((4, 4, t, f), BF)
    keep_i, give_i = pl.pallas_call(
        input_kernel,
        out_shape=(blocks, blocks),
        in_specs=[SMEM] + [HBM] * 3,
        out_specs=(HBM,) * 2,
        scratch_shapes=[
            pltpu.VMEM((4 * t, 2 * width), BF),
            pltpu.VMEM((d, 2 * width), BF),
            pltpu.VMEM((4, 4, t, f), BF),
            pltpu.VMEM((4, 4, t, f), BF),
            DMA((3,)),
            DMA((8,)),
        ],
        cost_estimate=pl.CostEstimate(flops=2 * 4 * t * d * 2 * width, bytes_accessed=1 << 23, transcendentals=0),
        name="input",
    )(core, pre_grad, whole, partner)
    got_i = shift(give_i, "c", 1)

    def part(offset):
        start = (0, at(offset), 0)
        return [lax.dynamic_slice(v, start, (2, brows, width)) for v in (keep, got_w)]

    fwd = shift(add(*part(4)), "z", 1)
    fwd, bwd = shift(add(fwd, *part(3)), "z", 1), shift(add(*part(-3)), "z", -1)
    fwd, bwd = shift(add(fwd, *part(2)), "z", 1), shift(add(bwd, *part(-2)), "z", -1)
    fwd, bwd = shift(add(fwd, *part(1)), "z", 1), shift(add(bwd, *part(-1)), "z", -1)
    block = add(fwd, bwd, *part(0))
    block = exchange(jnp.moveaxis(block.reshape(2, 4, rows, width), 1, 0), "y")
    block = jnp.moveaxis(block, 0, 2).reshape(2, rows, 4 * width).astype(F32)

    mine = scatter4([(keep_i[j], got_i[j]) for j in range(4)], 0)
    mine = [jnp.stack([mine[0][j], mine[1][j]]) for j in range(4)]
    mine = add(mine[0], *(ring(mine[j], j if j < 3 else -1, 1) for j in (2, 1, 3)))
    input_grad = jnp.concatenate([jnp.where(first, mine[0], mine[1]), jnp.where(first, mine[1], mine[0])], 0)
    return input_grad, block[0], block[1].T


def solution(mesh):
    split = Mesh(mesh.devices.reshape(8, 4, 4, 2), ("z", "y", "x", "c"))
    fs, tp = ("z", "y"), ("x", "c")
    in_specs = (P(fs, tp), P(fs, tp), P(fs, tp), P(tp, fs))
    out_specs = (P(fs, tp), P(fs, tp), P(tp, fs))

    return jax.shard_map(per_device, mesh=split, in_specs=in_specs, out_specs=out_specs, check_vma=False)
```

```python
import functools

import jax
import jax.numpy as jnp
from jax import lax
from jax.experimental import pallas as pl
from jax.experimental.pallas import tpu as pltpu
from jax.sharding import Mesh
from jax.sharding import PartitionSpec as P


BF = jnp.bfloat16
F32 = jnp.float32


def shift(value, axis, by):
    n = lax.axis_size(axis)
    return lax.ppermute(value, axis, [(i, (i + by) % n) for i in range(n)])


def ring(value, by, x_core, cross=False):
    ny, nx = lax.axis_size("y"), lax.axis_size("x")
    pairs = []
    for y in range(ny):
        for x in range(nx):
            for c in range(2):
                to = (y, (x + by) % nx) if c == x_core else ((y + by) % ny, x)
                pairs.append(((y * nx + x) * 2 + c, (to[0] * nx + to[1]) * 2 + (1 - c if cross else c)))
    return lax.ppermute(value, ("y", "x", "c"), pairs)


def exchange(value, axes):
    return lax.all_to_all(value, axes, split_axis=0, concat_axis=0, tiled=True)


def add(*terms):
    return sum(t.astype(F32) for t in terms).astype(BF)


def put(buf, value, *start):
    return lax.dynamic_update_slice(buf, value, start)


def dot(left, right, lc, rc):
    return lax.dot_general(left, right, (((lc,), (rc,)), ((), ())), preferred_element_type=F32)


def scatter4(terms, x_core):
    up = ring(terms[2][0], 1, x_core)
    down = ring(terms[2][1], -1, x_core)
    to_next = jnp.stack([add(terms[1][0], up), terms[1][1]])
    to_prev = jnp.stack([terms[3][0], add(terms[3][1], down)])
    a = ring(to_next, 1, x_core)
    b = ring(to_prev, -1, x_core)
    return [add(terms[0][i], a[i], b[i]) for i in range(2)]


def grads_kernel(core, own, succ, far, prev, theirs, their_far, own_w, other_w,
                 give, keep, pre_grad, xw, kw, ww, rect, act, pg, gives, keeps, sems, outs, *, scale):
    blocks, t, _ = xw.shape
    f, w = kw.shape[2], own_w.shape[2]
    is_first = core[0] == 0
    pairs = ((own, theirs.at[0]), (succ, theirs.at[1]), (far, their_far), (prev, theirs.at[2]))

    def weights(n):
        return [
            pltpu.make_async_copy(v.at[n], ww.at[n, :, pl.ds(k * w, w)], sems.at[2 * n + k])
            for k, v in enumerate((own_w, other_w))
        ]

    def tokens(core_0, which):
        for j, (mine, other) in enumerate(pairs):
            if which == 0:
                source, target = mine if core_0 else other, xw.at[:, :, pl.ds(j * f, f)]
            else:
                source, target = other if core_0 else mine, kw.at[:, pl.ds(j * t, t)]
            yield pltpu.make_async_copy(source, target, sems.at[4 + 4 * which + j])

    def start(core_0):
        for n in range(2):
            for copy in [*weights(n), *tokens(core_0, n)]:
                copy.start()

    @pl.when(is_first)
    def _():
        start(True)

    @pl.when(jnp.logical_not(is_first))
    def _():
        start(False)

    for copy in [*weights(0), *tokens(True, 0)]:
        copy.wait()

    def forward(i, carry):
        rect[i] = jnp.maximum(dot(xw[i], ww[0], 1, 0), 0.0)
        return carry

    lax.fori_loop(0, blocks, forward, 0)
    for copy in [*weights(1), *tokens(True, 1)]:
        copy.wait()

    def backward(i, carry):
        rows = pl.ds(i * t, t)
        ag = dot(kw[0, rows], ww[1, 0:f], 1, 0)
        for q in range(1, blocks):
            ag += dot(kw[q, rows], ww[1, q * f:(q + 1) * f], 1, 0)
        act[rows] = (rect[i] * rect[i]).astype(BF)
        pg[rows] = (2.0 * rect[i] * ag).astype(BF)
        return carry

    lax.fori_loop(0, blocks, backward, 0)
    copies = [pltpu.make_async_copy(pg, pre_grad, outs.at[0])]
    copies[0].start()

    def results(q, r):
        at = (slice(None), pl.ds(pl.multiple_of(q * f + r * w, w), w))
        pairs = ((gives, give), (keeps, keep))
        return [
            pltpu.make_async_copy(source.at[at], target.at[at], outs.at[1 + 2 * (q * (f // w) + r) + k])
            for k, (source, target) in enumerate(pairs)
        ]

    def features(q, carry):
        for r in range(f // w):
            cols = pl.ds(pl.multiple_of(q * f + r * w, w), w)
            up = dot(xw[:, :, cols].reshape(blocks * t, w), pg[...], 0, 0)
            down = dot(kw[q, :, r * w:(r + 1) * w], act[...], 0, 0)
            for n, part in enumerate((up, down)):
                part = (part * scale).astype(BF)
                keeps[n, cols], gives[n, cols] = part[:, :w], part[:, w:]
            for copy in results(q, r):
                copy.start()
        return carry

    lax.fori_loop(0, blocks, features, 0)
    for q in range(blocks):
        for r in range(f // w):
            copies += results(q, r)
    for copy in copies:
        copy.wait()


def input_kernel(core, pre_grad, own_w, other_w, keep, give, pg, uw, low, high, sems, outs):
    t, f = low.shape[2], low.shape[3]
    w = own_w.shape[2]
    is_first = core[0] == 0
    copies = [
        pltpu.make_async_copy(pre_grad, pg, sems.at[0]),
        pltpu.make_async_copy(own_w.at[0], uw.at[:, pl.ds(0, w)], sems.at[1]),
        pltpu.make_async_copy(other_w.at[0], uw.at[:, pl.ds(w, w)], sems.at[2]),
    ]
    for copy in copies:
        copy.start()
    for copy in copies:
        copy.wait()

    def results(j, core_0):
        a, b = (keep, give) if core_0 else (give, keep)
        return [
            pltpu.make_async_copy(low.at[j], a.at[j], outs.at[2 * j]),
            pltpu.make_async_copy(high.at[:, j], b.at[:, j], outs.at[2 * j + 1]),
        ]

    def features(j, carry):
        for k in range(2):
            right = uw[pl.ds((2 * j + k) * f, f)]
            for i in range(4):
                part = dot(pg[i * t:(i + 1) * t], right, 1, 1).astype(BF)
                if k == 0:
                    low[j, i] = part
                else:
                    high[i, j] = part

        @pl.when(is_first)
        def _():
            for copy in results(j, True):
                copy.start()

        @pl.when(jnp.logical_not(is_first))
        def _():
            for copy in results(j, False):
                copy.start()

        return carry

    lax.fori_loop(0, 4, features, 0)
    for j in range(4):
        for copy in results(j, True):
            copy.wait()


SMEM = pl.BlockSpec(memory_space=pltpu.SMEM)
HBM = pl.BlockSpec(memory_space=pltpu.HBM)
DMA = pltpu.SemaphoreType.DMA


def per_device(normed_input, cotangent, up_weight, down_weight):
    z, _, x, c = (lax.axis_index(a) for a in "zyxc")
    nz = lax.axis_size("z")
    tokens = normed_input.shape[0] * nz * lax.axis_size("y")
    scale = tokens ** -0.5
    t, f = normed_input.shape[0] // 2, normed_input.shape[1]
    first = c == 0
    core = c.reshape(1).astype(jnp.int32)

    swap = shift(jnp.where(first, cotangent, normed_input), "c", 1)

    rows, width = up_weight.shape[0], up_weight.shape[1] // 4
    pair = jnp.stack([up_weight, down_weight.T])
    quarters = jnp.moveaxis(pair.reshape(2, rows, 4, width), 2, 0)
    block = jnp.moveaxis(exchange(quarters, "y"), 0, 1).reshape(2, 4 * rows, width)
    brows = 4 * rows

    mine = jnp.concatenate(
        [jnp.where(first, normed_input, swap), jnp.where(first, swap, cotangent)], 1
    ).reshape(2, t, 2 * f)
    mine = jnp.where(first, mine, mine[::-1])
    prev, succ = ring(mine, 1, 1), ring(mine, -1, 1)
    stage = jnp.zeros((2, 4, t, 2 * f), BF)
    stage = put(stage, mine[:, None], 0, 0, 0, 0)
    far = prev[0], succ[1]
    far = ring(far[0], 1, 1), ring(far[1], -1, 1)
    stage = put(stage, prev[:, None], 0, 3, 0, 0)
    stage = put(stage, succ[:, None], 0, 1, 0, 0)
    stage = put(stage, far[0][None, None], 0, 2, 0, 0)
    stage = put(stage, far[1][None, None], 1, 2, 0, 0)
    prev, succ = ring(stage, 1, 0), ring(stage, -1, 0)
    far, their_far = ring(prev[0], 1, 0), ring(succ[1], -1, 0, cross=True)
    theirs = shift(jnp.stack([stage[1], succ[1], prev[1]]), "c", 1)
    own, succ, prev = stage[0], succ[0], prev[0]

    def at(offset):
        return (z + offset - 2 * x) % nz * brows

    def place(buf, value, offset):
        return put(buf, value, 0, at(offset), 0)

    whole = jnp.zeros((2, nz * brows, width), BF)
    whole = place(whole, block, 0)
    fwd, bwd = block, block
    for k in range(1, 4):
        fwd, bwd = shift(fwd, "z", 1), shift(bwd, "z", -1)
        whole = place(place(whole, fwd, -k), bwd, k)
    whole = place(whole, shift(fwd, "z", 1), 4)
    partner = shift(whole, "c", 1)

    d = nz * brows
    half = jax.ShapeDtypeStruct((2, d, width), BF)
    give, keep, pre_grad = pl.pallas_call(
        functools.partial(grads_kernel, scale=scale),
        out_shape=(half, half, jax.ShapeDtypeStruct((4 * t, 2 * width), BF)),
        in_specs=[SMEM] + [HBM] * 8,
        out_specs=(HBM,) * 3,
        scratch_shapes=[
            pltpu.VMEM((4, t, d), BF),
            pltpu.VMEM((4, 4 * t, 2 * f), BF),
            pltpu.VMEM((2, d, 2 * width), BF),
            pltpu.VMEM((4, t, 2 * width), F32),
            pltpu.VMEM((4 * t, 2 * width), BF),
            pltpu.VMEM((4 * t, 2 * width), BF),
            pltpu.VMEM((2, d, width), BF),
            pltpu.VMEM((2, d, width), BF),
            DMA((12,)),
            DMA((1 + 2 * (d // width),)),
        ],
        cost_estimate=pl.CostEstimate(flops=2 * 4 * 4 * t * d * 2 * width, bytes_accessed=1 << 24, transcendentals=0),
        name="grads",
    )(core, own, succ, far, prev, theirs, their_far, whole, partner)
    got_w = shift(give, "c", 1)

    blocks = jax.ShapeDtypeStruct((4, 4, t, f), BF)
    keep_i, give_i = pl.pallas_call(
        input_kernel,
        out_shape=(blocks, blocks),
        in_specs=[SMEM] + [HBM] * 3,
        out_specs=(HBM,) * 2,
        scratch_shapes=[
            pltpu.VMEM((4 * t, 2 * width), BF),
            pltpu.VMEM((d, 2 * width), BF),
            pltpu.VMEM((4, 4, t, f), BF),
            pltpu.VMEM((4, 4, t, f), BF),
            DMA((3,)),
            DMA((8,)),
        ],
        cost_estimate=pl.CostEstimate(flops=2 * 4 * t * d * 2 * width, bytes_accessed=1 << 23, transcendentals=0),
        name="input",
    )(core, pre_grad, whole, partner)
    got_i = shift(give_i, "c", 1)

    def part(offset):
        start = (0, at(offset), 0)
        return [lax.dynamic_slice(v, start, (2, brows, width)) for v in (keep, got_w)]

    fwd = shift(add(*part(4)), "z", 1)
    fwd, bwd = shift(add(fwd, *part(3)), "z", 1), shift(add(*part(-3)), "z", -1)
    fwd, bwd = shift(add(fwd, *part(2)), "z", 1), shift(add(bwd, *part(-2)), "z", -1)
    fwd, bwd = shift(add(fwd, *part(1)), "z", 1), shift(add(bwd, *part(-1)), "z", -1)
    block = add(fwd, bwd, *part(0))
    block = exchange(jnp.moveaxis(block.reshape(2, 4, rows, width), 1, 0), "y")
    block = jnp.moveaxis(block, 0, 2).reshape(2, rows, 4 * width).astype(F32)

    mine = scatter4([(keep_i[j], got_i[j]) for j in range(4)], 0)
    mine = [jnp.stack([mine[0][j], mine[1][j]]) for j in range(4)]
    mine = add(mine[0], *(ring(mine[j], j if j < 3 else -1, 1) for j in (2, 1, 3)))
    input_grad = jnp.concatenate([jnp.where(first, mine[0], mine[1]), jnp.where(first, mine[1], mine[0])], 0)
    return input_grad, block[0], block[1].T


def solution(mesh):
    split = Mesh(mesh.devices.reshape(8, 4, 4, 2), ("z", "y", "x", "c"))
    fs, tp = ("z", "y"), ("x", "c")
    in_specs = (P(fs, tp), P(fs, tp), P(fs, tp), P(tp, fs))
    out_specs = (P(fs, tp), P(fs, tp), P(tp, fs))

    return jax.shard_map(per_device, mesh=split, in_specs=in_specs, out_specs=out_specs, check_vma=False)
```

```python
import functools

import jax
import jax.numpy as jnp
from jax import lax
from jax.experimental import pallas as pl
from jax.experimental.pallas import tpu as pltpu
from jax.sharding import Mesh
from jax.sharding import PartitionSpec as P


BF = jnp.bfloat16
F32 = jnp.float32


def shift(value, axis, by):
    n = lax.axis_size(axis)
    return lax.ppermute(value, axis, [(i, (i + by) % n) for i in range(n)])


def ring(value, by, x_core, cross=False):
    ny, nx = lax.axis_size("y"), lax.axis_size("x")
    pairs = []
    for y in range(ny):
        for x in range(nx):
            for c in range(2):
                to = (y, (x + by) % nx) if c == x_core else ((y + by) % ny, x)
                pairs.append(((y * nx + x) * 2 + c, (to[0] * nx + to[1]) * 2 + (1 - c if cross else c)))
    return lax.ppermute(value, ("y", "x", "c"), pairs)


def exchange(value, axes):
    return lax.all_to_all(value, axes, split_axis=0, concat_axis=0, tiled=True)


def add(*terms):
    return sum(t.astype(F32) for t in terms).astype(BF)


def put(buf, value, *start):
    return lax.dynamic_update_slice(buf, value, start)


def dot(left, right, lc, rc):
    return lax.dot_general(left, right, (((lc,), (rc,)), ((), ())), preferred_element_type=F32)


def scatter4(terms, x_core):
    up = ring(terms[2][0], 1, x_core)
    down = ring(terms[2][1], -1, x_core)
    to_next = jnp.stack([add(terms[1][0], up), terms[1][1]])
    to_prev = jnp.stack([terms[3][0], add(terms[3][1], down)])
    a = ring(to_next, 1, x_core)
    b = ring(to_prev, -1, x_core)
    return [add(terms[0][i], a[i], b[i]) for i in range(2)]


def grads_kernel(core, own, succ, far, prev, theirs, their_succ, their_far, their_prev, own_w, other_w,
                 give, keep, pre_grad, xw, kw, ww, rect, act, pg, gives, keeps, sems, outs, *, scale):
    blocks, t, _ = xw.shape
    f, w = kw.shape[2], own_w.shape[2]
    is_first = core[0] == 0
    pairs = ((own, theirs), (succ, their_succ), (far, their_far), (prev, their_prev))

    def weights(n):
        return [
            pltpu.make_async_copy(v.at[n], ww.at[n, :, pl.ds(k * w, w)], sems.at[2 * n + k])
            for k, v in enumerate((own_w, other_w))
        ]

    def tokens(core_0, which):
        for j, (mine, other) in enumerate(pairs):
            if which == 0:
                source, target = mine if core_0 else other, xw.at[:, :, pl.ds(j * f, f)]
            else:
                source, target = other if core_0 else mine, kw.at[:, pl.ds(j * t, t)]
            yield pltpu.make_async_copy(source, target, sems.at[4 + 4 * which + j])

    def start(core_0):
        for n in range(2):
            for copy in [*weights(n), *tokens(core_0, n)]:
                copy.start()

    @pl.when(is_first)
    def _():
        start(True)

    @pl.when(jnp.logical_not(is_first))
    def _():
        start(False)

    for copy in [*weights(0), *tokens(True, 0)]:
        copy.wait()

    def forward(i, carry):
        rect[i] = jnp.maximum(dot(xw[i], ww[0], 1, 0), 0.0)
        return carry

    lax.fori_loop(0, blocks, forward, 0)
    for copy in [*weights(1), *tokens(True, 1)]:
        copy.wait()

    def backward(i, carry):
        rows = pl.ds(i * t, t)
        ag = dot(kw[0, rows], ww[1, 0:f], 1, 0)
        for q in range(1, blocks):
            ag += dot(kw[q, rows], ww[1, q * f:(q + 1) * f], 1, 0)
        act[rows] = (rect[i] * rect[i]).astype(BF)
        pg[rows] = (2.0 * rect[i] * ag).astype(BF)
        return carry

    lax.fori_loop(0, blocks, backward, 0)
    copies = [pltpu.make_async_copy(pg, pre_grad, outs.at[0])]
    copies[0].start()

    def results(q, r):
        at = (slice(None), pl.ds(pl.multiple_of(q * f + r * w, w), w))
        pairs = ((gives, give), (keeps, keep))
        return [
            pltpu.make_async_copy(source.at[at], target.at[at], outs.at[1 + 2 * (q * (f // w) + r) + k])
            for k, (source, target) in enumerate(pairs)
        ]

    def features(q, carry):
        for r in range(f // w):
            cols = pl.ds(pl.multiple_of(q * f + r * w, w), w)
            up = dot(xw[:, :, cols].reshape(blocks * t, w), pg[...], 0, 0)
            down = dot(kw[q, :, r * w:(r + 1) * w], act[...], 0, 0)
            for n, part in enumerate((up, down)):
                part = (part * scale).astype(BF)
                keeps[n, cols], gives[n, cols] = part[:, :w], part[:, w:]
            for copy in results(q, r):
                copy.start()
        return carry

    lax.fori_loop(0, blocks, features, 0)
    for q in range(blocks):
        for r in range(f // w):
            copies += results(q, r)
    for copy in copies:
        copy.wait()


def input_kernel(core, pre_grad, own_w, other_w, keep, give, pg, uw, low, high, sems, outs):
    t, f = low.shape[2], low.shape[3]
    w = own_w.shape[2]
    is_first = core[0] == 0
    copies = [
        pltpu.make_async_copy(pre_grad, pg, sems.at[0]),
        pltpu.make_async_copy(own_w.at[0], uw.at[:, pl.ds(0, w)], sems.at[1]),
        pltpu.make_async_copy(other_w.at[0], uw.at[:, pl.ds(w, w)], sems.at[2]),
    ]
    for copy in copies:
        copy.start()
    for copy in copies:
        copy.wait()

    def results(j, core_0):
        a, b = (keep, give) if core_0 else (give, keep)
        return [
            pltpu.make_async_copy(low.at[j], a.at[j], outs.at[2 * j]),
            pltpu.make_async_copy(high.at[:, j], b.at[:, j], outs.at[2 * j + 1]),
        ]

    def features(j, carry):
        for k in range(2):
            right = uw[pl.ds((2 * j + k) * f, f)]
            for i in range(4):
                part = dot(pg[i * t:(i + 1) * t], right, 1, 1).astype(BF)
                if k == 0:
                    low[j, i] = part
                else:
                    high[i, j] = part

        @pl.when(is_first)
        def _():
            for copy in results(j, True):
                copy.start()

        @pl.when(jnp.logical_not(is_first))
        def _():
            for copy in results(j, False):
                copy.start()

        return carry

    lax.fori_loop(0, 4, features, 0)
    for j in range(4):
        for copy in results(j, True):
            copy.wait()


SMEM = pl.BlockSpec(memory_space=pltpu.SMEM)
HBM = pl.BlockSpec(memory_space=pltpu.HBM)
DMA = pltpu.SemaphoreType.DMA


def per_device(normed_input, cotangent, up_weight, down_weight):
    z, _, x, c = (lax.axis_index(a) for a in "zyxc")
    nz = lax.axis_size("z")
    tokens = normed_input.shape[0] * nz * lax.axis_size("y")
    scale = tokens ** -0.5
    t, f = normed_input.shape[0] // 2, normed_input.shape[1]
    first = c == 0
    core = c.reshape(1).astype(jnp.int32)

    swap = shift(jnp.where(first, cotangent, normed_input), "c", 1)

    rows, width = up_weight.shape[0], up_weight.shape[1] // 4
    pair = jnp.stack([up_weight, down_weight.T])
    quarters = jnp.moveaxis(pair.reshape(2, rows, 4, width), 2, 0)
    block = jnp.moveaxis(exchange(quarters, "y"), 0, 1).reshape(2, 4 * rows, width)
    brows = 4 * rows

    mine = jnp.concatenate(
        [jnp.where(first, normed_input, swap), jnp.where(first, swap, cotangent)], 1
    ).reshape(2, t, 2 * f)
    mine = jnp.where(first, mine, mine[::-1])
    prev, succ = ring(mine, 1, 1), ring(mine, -1, 1)
    far = prev[0], succ[1]
    far = ring(far[0], 1, 1), ring(far[1], -1, 1)
    stage = []
    for h in range(2):
        blocks = jnp.zeros((4, t, 2 * f), BF)
        for j, block_j in ((0, mine[h]), (3, prev[h]), (1, succ[h]), (2, far[h])):
            blocks = put(blocks, block_j[None], j, 0, 0)
        stage.append(blocks)

    prev = ring(stage[0], 1, 0)
    their_succ = ring(stage[1], -1, 0, cross=True)
    succ = ring(stage[0], -1, 0)
    their_prev = ring(stage[1], 1, 0, cross=True)
    far, their_far = ring(prev, 1, 0), ring(their_succ, -1, 1)
    theirs = shift(stage[1], "c", 1)

    def at(offset):
        return (z + offset - 2 * x) % nz * brows

    def place(buf, value, offset):
        return put(buf, value, 0, at(offset), 0)

    whole = jnp.zeros((2, nz * brows, width), BF)
    whole = place(whole, block, 0)
    fwd, bwd = block, block
    for k in range(1, 4):
        fwd, bwd = shift(fwd, "z", 1), shift(bwd, "z", -1)
        whole = place(place(whole, fwd, -k), bwd, k)
    whole = place(whole, shift(fwd, "z", 1), 4)
    partner = shift(whole, "c", 1)

    d = nz * brows
    half = jax.ShapeDtypeStruct((2, d, width), BF)
    give, keep, pre_grad = pl.pallas_call(
        functools.partial(grads_kernel, scale=scale),
        out_shape=(half, half, jax.ShapeDtypeStruct((4 * t, 2 * width), BF)),
        in_specs=[SMEM] + [HBM] * 10,
        out_specs=(HBM,) * 3,
        scratch_shapes=[
            pltpu.VMEM((4, t, d), BF),
            pltpu.VMEM((4, 4 * t, 2 * f), BF),
            pltpu.VMEM((2, d, 2 * width), BF),
            pltpu.VMEM((4, t, 2 * width), F32),
            pltpu.VMEM((4 * t, 2 * width), BF),
            pltpu.VMEM((4 * t, 2 * width), BF),
            pltpu.VMEM((2, d, width), BF),
            pltpu.VMEM((2, d, width), BF),
            DMA((12,)),
            DMA((1 + 2 * (d // width),)),
        ],
        cost_estimate=pl.CostEstimate(flops=2 * 4 * 4 * t * d * 2 * width, bytes_accessed=1 << 24, transcendentals=0),
        name="grads",
    )(core, stage[0], succ, far, prev, theirs, their_succ, their_far, their_prev, whole, partner)
    got_w = shift(give, "c", 1)

    blocks = jax.ShapeDtypeStruct((4, 4, t, f), BF)
    keep_i, give_i = pl.pallas_call(
        input_kernel,
        out_shape=(blocks, blocks),
        in_specs=[SMEM] + [HBM] * 3,
        out_specs=(HBM,) * 2,
        scratch_shapes=[
            pltpu.VMEM((4 * t, 2 * width), BF),
            pltpu.VMEM((d, 2 * width), BF),
            pltpu.VMEM((4, 4, t, f), BF),
            pltpu.VMEM((4, 4, t, f), BF),
            DMA((3,)),
            DMA((8,)),
        ],
        cost_estimate=pl.CostEstimate(flops=2 * 4 * t * d * 2 * width, bytes_accessed=1 << 23, transcendentals=0),
        name="input",
    )(core, pre_grad, whole, partner)
    got_i = shift(give_i, "c", 1)

    def part(offset):
        start = (0, at(offset), 0)
        return [lax.dynamic_slice(v, start, (2, brows, width)) for v in (keep, got_w)]

    fwd = shift(add(*part(4)), "z", 1)
    fwd, bwd = shift(add(fwd, *part(3)), "z", 1), shift(add(*part(-3)), "z", -1)
    fwd, bwd = shift(add(fwd, *part(2)), "z", 1), shift(add(bwd, *part(-2)), "z", -1)
    fwd, bwd = shift(add(fwd, *part(1)), "z", 1), shift(add(bwd, *part(-1)), "z", -1)
    block = add(fwd, bwd, *part(0))
    block = exchange(jnp.moveaxis(block.reshape(2, 4, rows, width), 1, 0), "y")
    block = jnp.moveaxis(block, 0, 2).reshape(2, rows, 4 * width).astype(F32)

    mine = scatter4([(keep_i[j], got_i[j]) for j in range(4)], 0)
    mine = [jnp.stack([mine[0][j], mine[1][j]]) for j in range(4)]
    mine = add(mine[0], *(ring(mine[j], j if j < 3 else -1, 1) for j in (2, 1, 3)))
    input_grad = jnp.concatenate([jnp.where(first, mine[0], mine[1]), jnp.where(first, mine[1], mine[0])], 0)
    return input_grad, block[0], block[1].T


def solution(mesh):
    split = Mesh(mesh.devices.reshape(8, 4, 4, 2), ("z", "y", "x", "c"))
    fs, tp = ("z", "y"), ("x", "c")
    in_specs = (P(fs, tp), P(fs, tp), P(fs, tp), P(tp, fs))
    out_specs = (P(fs, tp), P(fs, tp), P(tp, fs))

    return jax.shard_map(per_device, mesh=split, in_specs=in_specs, out_specs=out_specs, check_vma=False)
```

```python
import functools

import jax
import jax.numpy as jnp
from jax import lax
from jax.experimental import pallas as pl
from jax.experimental.pallas import tpu as pltpu
from jax.sharding import Mesh
from jax.sharding import PartitionSpec as P


BF = jnp.bfloat16
F32 = jnp.float32


def shift(value, axis, by):
    n = lax.axis_size(axis)
    return lax.ppermute(value, axis, [(i, (i + by) % n) for i in range(n)])


def ring(value, by, x_core, cross=False):
    ny, nx = lax.axis_size("y"), lax.axis_size("x")
    pairs = []
    for y in range(ny):
        for x in range(nx):
            for c in range(2):
                to = (y, (x + by) % nx) if c == x_core else ((y + by) % ny, x)
                pairs.append(((y * nx + x) * 2 + c, (to[0] * nx + to[1]) * 2 + (1 - c if cross else c)))
    return lax.ppermute(value, ("y", "x", "c"), pairs)


def exchange(value, axes):
    return lax.all_to_all(value, axes, split_axis=0, concat_axis=0, tiled=True)


def add(*terms):
    return sum(t.astype(F32) for t in terms).astype(BF)


def put(buf, value, *start):
    return lax.dynamic_update_slice(buf, value, start)


def dot(left, right, lc, rc):
    return lax.dot_general(left, right, (((lc,), (rc,)), ((), ())), preferred_element_type=F32)


def scatter4(terms, x_core):
    up = ring(terms[2][0], 1, x_core)
    down = ring(terms[2][1], -1, x_core)
    to_next = jnp.stack([add(terms[1][0], up), terms[1][1]])
    to_prev = jnp.stack([terms[3][0], add(terms[3][1], down)])
    a = ring(to_next, 1, x_core)
    b = ring(to_prev, -1, x_core)
    return [add(terms[0][i], a[i], b[i]) for i in range(2)]


def grads_kernel(core, own, succ, far, prev, theirs, their_succ, their_far, their_prev, own_w, other_w,
                 give, keep, pre_grad, xw, kw, ww, rect, act, pg, gives, keeps, sems, outs, *, scale):
    blocks, t, _ = xw.shape
    f, w = kw.shape[2], own_w.shape[2]
    is_first = core[0] == 0
    pairs = ((own, theirs), (succ, their_succ), (far, their_far), (prev, their_prev))

    def weights(n):
        return [
            pltpu.make_async_copy(v.at[n], ww.at[n, :, pl.ds(k * w, w)], sems.at[2 * n + k])
            for k, v in enumerate((own_w, other_w))
        ]

    def tokens(core_0, which):
        for j, (mine, other) in enumerate(pairs):
            if which == 0:
                source, target = mine if core_0 else other, xw.at[:, :, pl.ds(j * f, f)]
            else:
                source, target = other if core_0 else mine, kw.at[:, pl.ds(j * t, t)]
            yield pltpu.make_async_copy(source, target, sems.at[4 + 4 * which + j])

    def start(core_0):
        for n in range(2):
            for copy in [*weights(n), *tokens(core_0, n)]:
                copy.start()

    @pl.when(is_first)
    def _():
        start(True)

    @pl.when(jnp.logical_not(is_first))
    def _():
        start(False)

    for copy in [*weights(0), *tokens(True, 0)]:
        copy.wait()

    def forward(i, carry):
        rect[i] = jnp.maximum(dot(xw[i], ww[0], 1, 0), 0.0)
        return carry

    lax.fori_loop(0, blocks, forward, 0)
    for copy in [*weights(1), *tokens(True, 1)]:
        copy.wait()

    def backward(i, carry):
        rows = pl.ds(i * t, t)
        ag = dot(kw[0, rows], ww[1, 0:f], 1, 0)
        for q in range(1, blocks):
            ag += dot(kw[q, rows], ww[1, q * f:(q + 1) * f], 1, 0)
        act[rows] = (rect[i] * rect[i]).astype(BF)
        pg[rows] = (2.0 * rect[i] * ag).astype(BF)
        return carry

    lax.fori_loop(0, blocks, backward, 0)
    copies = [pltpu.make_async_copy(pg, pre_grad, outs.at[0])]
    copies[0].start()

    def results(q, r):
        at = (slice(None), pl.ds(pl.multiple_of(q * f + r * w, w), w))
        pairs = ((gives, give), (keeps, keep))
        return [
            pltpu.make_async_copy(source.at[at], target.at[at], outs.at[1 + 2 * (q * (f // w) + r) + k])
            for k, (source, target) in enumerate(pairs)
        ]

    def features(q, carry):
        for r in range(f // w):
            cols = pl.ds(pl.multiple_of(q * f + r * w, w), w)
            up = dot(xw[:, :, cols].reshape(blocks * t, w), pg[...], 0, 0)
            down = dot(kw[q, :, r * w:(r + 1) * w], act[...], 0, 0)
            for n, part in enumerate((up, down)):
                part = (part * scale).astype(BF)
                keeps[n, cols], gives[n, cols] = part[:, :w], part[:, w:]
            for copy in results(q, r):
                copy.start()
        return carry

    lax.fori_loop(0, blocks, features, 0)
    for q in range(blocks):
        for r in range(f // w):
            copies += results(q, r)
    for copy in copies:
        copy.wait()


def input_kernel(core, pre_grad, own_w, other_w, keep, give, pg, uw, low, high, sems, outs):
    t, f = low.shape[2], low.shape[3]
    w = own_w.shape[2]
    is_first = core[0] == 0
    copies = [
        pltpu.make_async_copy(pre_grad, pg, sems.at[0]),
        pltpu.make_async_copy(own_w.at[0], uw.at[:, pl.ds(0, w)], sems.at[1]),
        pltpu.make_async_copy(other_w.at[0], uw.at[:, pl.ds(w, w)], sems.at[2]),
    ]
    for copy in copies:
        copy.start()
    for copy in copies:
        copy.wait()

    def results(j, core_0):
        a, b = (keep, give) if core_0 else (give, keep)
        return [
            pltpu.make_async_copy(low.at[j], a.at[j], outs.at[2 * j]),
            pltpu.make_async_copy(high.at[:, j], b.at[:, j], outs.at[2 * j + 1]),
        ]

    def features(j, carry):
        for k in range(2):
            right = uw[pl.ds((2 * j + k) * f, f)]
            for i in range(4):
                part = dot(pg[i * t:(i + 1) * t], right, 1, 1).astype(BF)
                if k == 0:
                    low[j, i] = part
                else:
                    high[i, j] = part

        @pl.when(is_first)
        def _():
            for copy in results(j, True):
                copy.start()

        @pl.when(jnp.logical_not(is_first))
        def _():
            for copy in results(j, False):
                copy.start()

        return carry

    lax.fori_loop(0, 4, features, 0)
    for j in range(4):
        for copy in results(j, True):
            copy.wait()


SMEM = pl.BlockSpec(memory_space=pltpu.SMEM)
HBM = pl.BlockSpec(memory_space=pltpu.HBM)
DMA = pltpu.SemaphoreType.DMA


def per_device(normed_input, cotangent, up_weight, down_weight):
    z, y, x, c = (lax.axis_index(a) for a in "zyxc")
    nz = lax.axis_size("z")
    tokens = normed_input.shape[0] * nz * lax.axis_size("y")
    scale = tokens ** -0.5
    t, f = normed_input.shape[0] // 2, normed_input.shape[1]
    first = c == 0
    core = c.reshape(1).astype(jnp.int32)

    swap = shift(jnp.where(first, cotangent, normed_input), "c", 1)

    rows, width = up_weight.shape[0], up_weight.shape[1] // 4
    pair = jnp.stack([up_weight, down_weight.T])
    quarters = jnp.moveaxis(pair.reshape(2, rows, 4, width), 2, 0)
    block = jnp.moveaxis(exchange(quarters, "y"), 0, 1).reshape(2, 4 * rows, width)
    brows = 4 * rows

    mine = jnp.concatenate(
        [jnp.where(first, normed_input, swap), jnp.where(first, swap, cotangent)], 1
    ).reshape(2, t, 2 * f)
    mine = jnp.where(first, mine, mine[::-1])
    prev, succ = ring(mine, 1, 1), ring(mine, -1, 1)
    far = prev[0], succ[1]
    far = ring(far[0], 1, 1), ring(far[1], -1, 1)
    stage = []
    for h in range(2):
        blocks = jnp.zeros((4, t, 2 * f), BF)
        for j, block_j in ((0, mine[h]), (3, prev[h]), (1, succ[h]), (2, far[h])):
            blocks = put(blocks, block_j[None], j, 0, 0)
        stage.append(blocks)

    prev = ring(stage[0], 1, 0)
    their_succ = ring(stage[1], -1, 0, cross=True)
    succ = ring(stage[0], -1, 0)
    their_prev = ring(stage[1], 1, 0, cross=True)
    far, their_far = ring(prev, 1, 0), ring(their_succ, -1, 1)
    theirs = shift(stage[1], "c", 1)

    def at(offset):
        return (z + offset - 2 * x) % nz * brows

    def place(buf, value, offset):
        return put(buf, value, 0, at(offset), 0)

    whole = jnp.zeros((2, nz * brows, width), BF)
    whole = place(whole, block, 0)
    fwd, bwd = block, block
    for k in range(1, 4):
        fwd, bwd = shift(fwd, "z", 1), shift(bwd, "z", -1)
        whole = place(place(whole, fwd, -k), bwd, k)
    whole = place(whole, shift(fwd, "z", 1), 4)
    partner = shift(whole, "c", 1)

    d = nz * brows
    half = jax.ShapeDtypeStruct((2, d, width), BF)
    give, keep, pre_grad = pl.pallas_call(
        functools.partial(grads_kernel, scale=scale),
        out_shape=(half, half, jax.ShapeDtypeStruct((4 * t, 2 * width), BF)),
        in_specs=[SMEM] + [HBM] * 10,
        out_specs=(HBM,) * 3,
        scratch_shapes=[
            pltpu.VMEM((4, t, d), BF),
            pltpu.VMEM((4, 4 * t, 2 * f), BF),
            pltpu.VMEM((2, d, 2 * width), BF),
            pltpu.VMEM((4, t, 2 * width), F32),
            pltpu.VMEM((4 * t, 2 * width), BF),
            pltpu.VMEM((4 * t, 2 * width), BF),
            pltpu.VMEM((2, d, width), BF),
            pltpu.VMEM((2, d, width), BF),
            DMA((12,)),
            DMA((1 + 2 * (d // width),)),
        ],
        cost_estimate=pl.CostEstimate(flops=2 * 4 * 4 * t * d * 2 * width, bytes_accessed=1 << 24, transcendentals=0),
        name="grads",
    )(core, stage[0], succ, far, prev, theirs, their_succ, their_far, their_prev, whole, partner)
    got_w = shift(give, "c", 1)

    blocks = jax.ShapeDtypeStruct((4, 4, t, f), BF)
    keep_i, give_i = pl.pallas_call(
        input_kernel,
        out_shape=(blocks, blocks),
        in_specs=[SMEM] + [HBM] * 3,
        out_specs=(HBM,) * 2,
        scratch_shapes=[
            pltpu.VMEM((4 * t, 2 * width), BF),
            pltpu.VMEM((d, 2 * width), BF),
            pltpu.VMEM((4, 4, t, f), BF),
            pltpu.VMEM((4, 4, t, f), BF),
            DMA((3,)),
            DMA((8,)),
        ],
        cost_estimate=pl.CostEstimate(flops=2 * 4 * t * d * 2 * width, bytes_accessed=1 << 23, transcendentals=0),
        name="input",
    )(core, pre_grad, whole, partner)
    got_i = shift(give_i, "c", 1)

    def part(offset):
        start = (0, at(offset), 0)
        return [lax.dynamic_slice(v, start, (2, brows, width)) for v in (keep, got_w)]

    fwd = shift(add(*part(4)), "z", 1)
    fwd, bwd = shift(add(fwd, *part(3)), "z", 1), shift(add(*part(-3)), "z", -1)
    fwd, bwd = shift(add(fwd, *part(2)), "z", 1), shift(add(bwd, *part(-2)), "z", -1)
    fwd, bwd = shift(add(fwd, *part(1)), "z", 1), shift(add(bwd, *part(-1)), "z", -1)
    block = add(fwd, bwd, *part(0))
    block = block.reshape(2, 4, rows, width)

    def row_block(k):
        return lax.dynamic_index_in_dim(block, (y + k) % 4, 1, keepdims=False)

    quarters = jnp.stack([row_block(0), *(shift(row_block(k), "y", k) for k in (1, 2, 3))])
    block = [lax.dynamic_index_in_dim(quarters, (y - q) % 4, 0, keepdims=False) for q in range(4)]
    block = jnp.concatenate(block, axis=2).astype(F32)

    mine = scatter4([(keep_i[j], got_i[j]) for j in range(4)], 0)
    mine = [jnp.stack([mine[0][j], mine[1][j]]) for j in range(4)]
    mine = add(mine[0], *(ring(mine[j], j if j < 3 else -1, 1) for j in (2, 1, 3)))
    input_grad = jnp.concatenate([jnp.where(first, mine[0], mine[1]), jnp.where(first, mine[1], mine[0])], 0)
    return input_grad, block[0], block[1].T


def solution(mesh):
    split = Mesh(mesh.devices.reshape(8, 4, 4, 2), ("z", "y", "x", "c"))
    fs, tp = ("z", "y"), ("x", "c")
    in_specs = (P(fs, tp), P(fs, tp), P(fs, tp), P(tp, fs))
    out_specs = (P(fs, tp), P(fs, tp), P(tp, fs))

    return jax.shard_map(per_device, mesh=split, in_specs=in_specs, out_specs=out_specs, check_vma=False)
```

```python
import functools

import jax
import jax.numpy as jnp
from jax import lax
from jax.experimental import pallas as pl
from jax.experimental.pallas import tpu as pltpu
from jax.sharding import Mesh
from jax.sharding import PartitionSpec as P


BF = jnp.bfloat16
F32 = jnp.float32


def shift(value, axis, by):
    n = lax.axis_size(axis)
    return lax.ppermute(value, axis, [(i, (i + by) % n) for i in range(n)])


def ring(value, by, x_core, cross=False):
    ny, nx = lax.axis_size("y"), lax.axis_size("x")
    pairs = []
    for y in range(ny):
        for x in range(nx):
            for c in range(2):
                to = (y, (x + by) % nx) if c == x_core else ((y + by) % ny, x)
                pairs.append(((y * nx + x) * 2 + c, (to[0] * nx + to[1]) * 2 + (1 - c if cross else c)))
    return lax.ppermute(value, ("y", "x", "c"), pairs)


def exchange(value, axes):
    return lax.all_to_all(value, axes, split_axis=0, concat_axis=0, tiled=True)


def add(*terms):
    return sum(t.astype(F32) for t in terms).astype(BF)


def put(buf, value, *start):
    return lax.dynamic_update_slice(buf, value, start)


def dot(left, right, lc, rc):
    return lax.dot_general(left, right, (((lc,), (rc,)), ((), ())), preferred_element_type=F32)


def scatter4(terms, x_core):
    up = ring(terms[2][0], 1, x_core)
    down = ring(terms[2][1], -1, x_core)
    to_next = jnp.stack([add(terms[1][0], up), terms[1][1]])
    to_prev = jnp.stack([terms[3][0], add(terms[3][1], down)])
    a = ring(to_next, 1, x_core)
    b = ring(to_prev, -1, x_core)
    return [add(terms[0][i], a[i], b[i]) for i in range(2)]


def grads_kernel(core, own, succ, far, prev, theirs, their_succ, their_far, their_prev, own_w, other_w,
                 give, pre_grad, act_out, xw, kw, ww, rect, act, pg, gives, sems, outs, *, scale):
    blocks, t, _ = xw.shape
    f, w = kw.shape[2], own_w.shape[2]
    is_first = core[0] == 0
    pairs = ((own, theirs), (succ, their_succ), (far, their_far), (prev, their_prev))

    def weights(n):
        return [
            pltpu.make_async_copy(v.at[n], ww.at[n, :, pl.ds(k * w, w)], sems.at[2 * n + k])
            for k, v in enumerate((own_w, other_w))
        ]

    def tokens(core_0, which):
        for j, (mine, other) in enumerate(pairs):
            if which == 0:
                source, target = mine if core_0 else other, xw.at[:, :, pl.ds(j * f, f)]
            else:
                source, target = other if core_0 else mine, kw.at[:, pl.ds(j * t, t)]
            yield pltpu.make_async_copy(source, target, sems.at[4 + 4 * which + j])

    def start(core_0):
        for n in range(2):
            for copy in [*weights(n), *tokens(core_0, n)]:
                copy.start()

    @pl.when(is_first)
    def _():
        start(True)

    @pl.when(jnp.logical_not(is_first))
    def _():
        start(False)

    for copy in [*weights(0), *tokens(True, 0)]:
        copy.wait()

    def forward(i, carry):
        rect[i] = jnp.maximum(dot(xw[i], ww[0], 1, 0), 0.0)
        return carry

    lax.fori_loop(0, blocks, forward, 0)
    for copy in [*weights(1), *tokens(True, 1)]:
        copy.wait()

    def backward(i, carry):
        rows = pl.ds(i * t, t)
        ag = dot(kw[0, rows], ww[1, 0:f], 1, 0)
        for q in range(1, blocks):
            ag += dot(kw[q, rows], ww[1, q * f:(q + 1) * f], 1, 0)
        act[rows] = (rect[i] * rect[i]).astype(BF)
        pg[rows] = (2.0 * rect[i] * ag).astype(BF)
        return carry

    lax.fori_loop(0, blocks, backward, 0)
    copies = [pltpu.make_async_copy(pg, pre_grad, outs.at[0]), pltpu.make_async_copy(act, act_out, outs.at[1])]
    for copy in copies:
        copy.start()

    def result(q, r):
        at = (slice(None), pl.ds(pl.multiple_of(q * f + r * w, w), w))
        return pltpu.make_async_copy(gives.at[at], give.at[at], outs.at[2 + q * (f // w) + r])

    def features(q, carry):
        for r in range(f // w):
            cols = pl.ds(pl.multiple_of(q * f + r * w, w), w)
            up = dot(xw[:, :, cols].reshape(blocks * t, w), pg[:, w:], 0, 0)
            down = dot(kw[q, :, r * w:(r + 1) * w], act[:, w:], 0, 0)
            gives[0, cols], gives[1, cols] = (up * scale).astype(BF), (down * scale).astype(BF)
            result(q, r).start()
        return carry

    lax.fori_loop(0, blocks, features, 0)
    for q in range(blocks):
        for r in range(f // w):
            copies.append(result(q, r))
    for copy in copies:
        copy.wait()


def own_kernel(core, own, succ, far, prev, theirs, their_succ, their_far, their_prev, pre_grad, act_in,
               keep, xw, kw, pg, act, keeps, sems, outs, *, scale):
    blocks, t, _ = xw.shape
    f, w = kw.shape[2], pg.shape[1]
    is_first = core[0] == 0
    pairs = ((own, theirs), (succ, their_succ), (far, their_far), (prev, their_prev))
    left = [
        pltpu.make_async_copy(pre_grad.at[:, pl.ds(0, w)], pg, sems.at[8]),
        pltpu.make_async_copy(act_in.at[:, pl.ds(0, w)], act, sems.at[9]),
    ]

    def tokens(core_0, which):
        for j, (mine, other) in enumerate(pairs):
            if which == 0:
                source, target = mine if core_0 else other, xw.at[:, :, pl.ds(j * f, f)]
            else:
                source, target = other if core_0 else mine, kw.at[:, pl.ds(j * t, t)]
            yield pltpu.make_async_copy(source, target, sems.at[4 * which + j])

    def start(core_0):
        for n in range(2):
            for copy in [left[n], *tokens(core_0, n)]:
                copy.start()

    @pl.when(is_first)
    def _():
        start(True)

    @pl.when(jnp.logical_not(is_first))
    def _():
        start(False)

    def result(n, q):
        at = (n, pl.ds(pl.multiple_of(q * f, f), f))
        return pltpu.make_async_copy(keeps.at[at], keep.at[at], outs.at[4 * n + q])

    for n in range(2):
        for copy in [left[n], *tokens(True, n)]:
            copy.wait()

        def features(q, carry):
            for r in range(f // w):
                cols = pl.ds(pl.multiple_of(q * f + r * w, w), w)
                if n == 0:
                    part = dot(xw[:, :, cols].reshape(blocks * t, w), pg[...], 0, 0)
                else:
                    part = dot(kw[q, :, r * w:(r + 1) * w], act[...], 0, 0)
                keeps[n, cols] = (part * scale).astype(BF)
            result(n, q).start()
            return carry

        lax.fori_loop(0, blocks, features, 0)
    for n in range(2):
        for q in range(blocks):
            result(n, q).wait()


def input_kernel(core, pre_grad, own_w, other_w, keep, give, pg, uw, low, high, sems, outs):
    t, f = low.shape[2], low.shape[3]
    w = own_w.shape[2]
    is_first = core[0] == 0
    copies = [
        pltpu.make_async_copy(pre_grad, pg, sems.at[0]),
        pltpu.make_async_copy(own_w.at[0], uw.at[:, pl.ds(0, w)], sems.at[1]),
        pltpu.make_async_copy(other_w.at[0], uw.at[:, pl.ds(w, w)], sems.at[2]),
    ]
    for copy in copies:
        copy.start()
    for copy in copies:
        copy.wait()

    def results(j, core_0):
        a, b = (keep, give) if core_0 else (give, keep)
        return [
            pltpu.make_async_copy(low.at[j], a.at[j], outs.at[2 * j]),
            pltpu.make_async_copy(high.at[:, j], b.at[:, j], outs.at[2 * j + 1]),
        ]

    def features(j, carry):
        for k in range(2):
            right = uw[pl.ds((2 * j + k) * f, f)]
            for i in range(4):
                part = dot(pg[i * t:(i + 1) * t], right, 1, 1).astype(BF)
                if k == 0:
                    low[j, i] = part
                else:
                    high[i, j] = part

        @pl.when(is_first)
        def _():
            for copy in results(j, True):
                copy.start()

        @pl.when(jnp.logical_not(is_first))
        def _():
            for copy in results(j, False):
                copy.start()

        return carry

    lax.fori_loop(0, 4, features, 0)
    for j in range(4):
        for copy in results(j, True):
            copy.wait()


SMEM = pl.BlockSpec(memory_space=pltpu.SMEM)
HBM = pl.BlockSpec(memory_space=pltpu.HBM)
DMA = pltpu.SemaphoreType.DMA


def per_device(normed_input, cotangent, up_weight, down_weight):
    z, y, x, c = (lax.axis_index(a) for a in "zyxc")
    nz = lax.axis_size("z")
    tokens = normed_input.shape[0] * nz * lax.axis_size("y")
    scale = tokens ** -0.5
    t, f = normed_input.shape[0] // 2, normed_input.shape[1]
    first = c == 0
    core = c.reshape(1).astype(jnp.int32)

    swap = shift(jnp.where(first, cotangent, normed_input), "c", 1)

    rows, width = up_weight.shape[0], up_weight.shape[1] // 4
    pair = jnp.stack([up_weight, down_weight.T])
    quarters = jnp.moveaxis(pair.reshape(2, rows, 4, width), 2, 0)
    block = jnp.moveaxis(exchange(quarters, "y"), 0, 1).reshape(2, 4 * rows, width)
    brows = 4 * rows

    mine = jnp.concatenate(
        [jnp.where(first, normed_input, swap), jnp.where(first, swap, cotangent)], 1
    ).reshape(2, t, 2 * f)
    mine = jnp.where(first, mine, mine[::-1])
    prev, succ = ring(mine, 1, 1), ring(mine, -1, 1)
    far = prev[0], succ[1]
    far = ring(far[0], 1, 1), ring(far[1], -1, 1)
    stage = []
    for h in range(2):
        blocks = jnp.zeros((4, t, 2 * f), BF)
        for j, block_j in ((0, mine[h]), (3, prev[h]), (1, succ[h]), (2, far[h])):
            blocks = put(blocks, block_j[None], j, 0, 0)
        stage.append(blocks)

    prev = ring(stage[0], 1, 0)
    their_succ = ring(stage[1], -1, 0, cross=True)
    succ = ring(stage[0], -1, 0)
    their_prev = ring(stage[1], 1, 0, cross=True)
    far, their_far = ring(prev, 1, 0), ring(their_succ, -1, 1)
    theirs = shift(stage[1], "c", 1)

    def at(offset):
        return (z + offset - 2 * x) % nz * brows

    def place(buf, value, offset):
        return put(buf, value, 0, at(offset), 0)

    whole = jnp.zeros((2, nz * brows, width), BF)
    whole = place(whole, block, 0)
    fwd, bwd = block, block
    for k in range(1, 4):
        fwd, bwd = shift(fwd, "z", 1), shift(bwd, "z", -1)
        whole = place(place(whole, fwd, -k), bwd, k)
    whole = place(whole, shift(fwd, "z", 1), 4)
    partner = shift(whole, "c", 1)

    d = nz * brows
    half = jax.ShapeDtypeStruct((2, d, width), BF)
    tokens_in = (stage[0], succ, far, prev, theirs, their_succ, their_far, their_prev)
    left = jax.ShapeDtypeStruct((4 * t, 2 * width), BF)
    buffers = [pltpu.VMEM((4, t, d), BF), pltpu.VMEM((4, 4 * t, 2 * f), BF)]
    give, pre_grad, act = pl.pallas_call(
        functools.partial(grads_kernel, scale=scale),
        out_shape=(half, left, left),
        in_specs=[SMEM] + [HBM] * 10,
        out_specs=(HBM,) * 3,
        scratch_shapes=[
            *buffers,
            pltpu.VMEM((2, d, 2 * width), BF),
            pltpu.VMEM((4, t, 2 * width), F32),
            pltpu.VMEM((4 * t, 2 * width), BF),
            pltpu.VMEM((4 * t, 2 * width), BF),
            pltpu.VMEM((2, d, width), BF),
            DMA((12,)),
            DMA((2 + d // width,)),
        ],
        cost_estimate=pl.CostEstimate(flops=2 * 3 * 4 * t * d * 2 * width, bytes_accessed=1 << 24, transcendentals=0),
        name="grads",
    )(core, *tokens_in, whole, partner)
    keep = pl.pallas_call(
        functools.partial(own_kernel, scale=scale),
        out_shape=half,
        in_specs=[SMEM] + [HBM] * 10,
        out_specs=HBM,
        scratch_shapes=[
            *buffers,
            pltpu.VMEM((4 * t, width), BF),
            pltpu.VMEM((4 * t, width), BF),
            pltpu.VMEM((2, d, width), BF),
            DMA((10,)),
            DMA((8,)),
        ],
        cost_estimate=pl.CostEstimate(flops=2 * 4 * t * d * 2 * width, bytes_accessed=1 << 24, transcendentals=0),
        name="ownhalf",
    )(core, *tokens_in, pre_grad, act)
    got_w = shift(give, "c", 1)

    blocks = jax.ShapeDtypeStruct((4, 4, t, f), BF)
    keep_i, give_i = pl.pallas_call(
        input_kernel,
        out_shape=(blocks, blocks),
        in_specs=[SMEM] + [HBM] * 3,
        out_specs=(HBM,) * 2,
        scratch_shapes=[
            pltpu.VMEM((4 * t, 2 * width), BF),
            pltpu.VMEM((d, 2 * width), BF),
            pltpu.VMEM((4, 4, t, f), BF),
            pltpu.VMEM((4, 4, t, f), BF),
            DMA((3,)),
            DMA((8,)),
        ],
        cost_estimate=pl.CostEstimate(flops=2 * 4 * t * d * 2 * width, bytes_accessed=1 << 23, transcendentals=0),
        name="input",
    )(core, pre_grad, whole, partner)
    got_i = shift(give_i, "c", 1)

    def part(offset):
        start = (0, at(offset), 0)
        return [lax.dynamic_slice(v, start, (2, brows, width)) for v in (keep, got_w)]

    fwd = shift(add(*part(4)), "z", 1)
    fwd, bwd = shift(add(fwd, *part(3)), "z", 1), shift(add(*part(-3)), "z", -1)
    fwd, bwd = shift(add(fwd, *part(2)), "z", 1), shift(add(bwd, *part(-2)), "z", -1)
    fwd, bwd = shift(add(fwd, *part(1)), "z", 1), shift(add(bwd, *part(-1)), "z", -1)
    block = add(fwd, bwd, *part(0))
    block = block.reshape(2, 4, rows, width)

    def row_block(k):
        return lax.dynamic_index_in_dim(block, (y + k) % 4, 1, keepdims=False)

    quarters = jnp.stack([row_block(0), *(shift(row_block(k), "y", k) for k in (1, 2, 3))])
    block = [lax.dynamic_index_in_dim(quarters, (y - q) % 4, 0, keepdims=False) for q in range(4)]
    block = jnp.concatenate(block, axis=2).astype(F32)

    mine = scatter4([(keep_i[j], got_i[j]) for j in range(4)], 0)
    mine = [jnp.stack([mine[0][j], mine[1][j]]) for j in range(4)]
    mine = add(mine[0], *(ring(mine[j], j if j < 3 else -1, 1) for j in (2, 1, 3)))
    input_grad = jnp.concatenate([jnp.where(first, mine[0], mine[1]), jnp.where(first, mine[1], mine[0])], 0)
    return input_grad, block[0], block[1].T


def solution(mesh):
    split = Mesh(mesh.devices.reshape(8, 4, 4, 2), ("z", "y", "x", "c"))
    fs, tp = ("z", "y"), ("x", "c")
    in_specs = (P(fs, tp), P(fs, tp), P(fs, tp), P(tp, fs))
    out_specs = (P(fs, tp), P(fs, tp), P(tp, fs))

    return jax.shard_map(per_device, mesh=split, in_specs=in_specs, out_specs=out_specs, check_vma=False)
```
